32 devices in a mesh: ep: 8 (over z, x), tp: 4 (over y, core).
Axes of the slice: x: 2, y: 2, z: 4, core: 2. Of those that a mesh axis runs over, the one named last changes fastest.
Arguments:
- queries: bfloat16 [4096, 1024], P('ep', 'tp'), may hold values from -6 to 6
- key_input: bfloat16 [4096, 256], P('ep'), may hold values from -6 to 6
- value_input: bfloat16 [4096, 256], P('ep'), may hold values from -6 to 6
- query_gain: float32 [64], replicated, may hold values from 0.1 to 1.9
- key_gain: float32 [64], replicated, may hold values from 0.1 to 1.9
- mix_out_weight: bfloat16 [1024, 2048], P('tp'), may hold values from -0.1875 to 0.1875
- expert_input: bfloat16 [1280, 2048], P('ep'), may hold values from -6 to 6
- ffn_gain: float32 [2048], replicated, may hold values from 0.1 to 1.9
- routes: int32 [1280, 2], P('ep'), may hold values from 0 to 7, all different within a row; in each aligned block of 160 rows (0 to 159, 160 to 319, ...) at most 60 rows name the same one
- route_scores: float32 [1280, 2], P('ep'), may hold values from 0.1 to 1
- gate_weight: bfloat16 [8, 2048, 4096], P('ep', None, 'tp'), may hold values from -0.125 to 0.125
- up_weight: bfloat16 [8, 2048, 4096], P('ep', None, 'tp'), may hold values from -0.125 to 0.125
- down_weight: bfloat16 [8, 4096, 2048], P('ep', 'tp'), may hold values from -0.09375 to 0.09375
Outputs:
- mixed_rows: bfloat16 [4096, 2048], P(('ep', 'tp'))
- expert_out: bfloat16 [1280, 2048], P('ep', 'tp')
The draws below stay inside these ranges and needn't reach their ends.
Inputs may be any that keep to these rules, and one draw needn't show every extreme that they name: `routes`: each row names 2 different experts. Within the rows of one index of ep (aligned blocks of 160 rows) no expert is named by more than 60 rows, and in every draw some expert is named by exactly 60 rows of some block.
All inputs are finite; a program needn't handle non-finite values.
Results may differ from the reference program's by a relative error of at most 0.019.
The reference program's roundings to bfloat16 on the way count: a program that leaves them out, or rounds other values in their place, can miss the bound.
Values may be sent and summed in bfloat16 or wider, within the bound.
A program may use at most 64 MiB of HBM per device.

```python
import math
import jax
import jax.numpy as jnp
import numpy as np
from jax import lax

D = 2048
HEADS = 16
KV_HEADS = 4
HD = 64
GRID_W = 64
FF = 4096
TOPK = 2
TOK2 = 160
EXPERTS = 8
CAP = 60
TOKENS1 = 4096
TOKENS2 = 1280
N_EP = 8
N_TP = 4


def block_levels(rng, dims, shards, least, top_value):
    loudness = 1.0
    for dim, parts in shards:
        heights = jax.random.uniform(jax.random.fold_in(jax.random.fold_in(rng, 6), dim), (parts,), jnp.float32, least / len(shards), top_value / len(shards))
        loudness = loudness * jnp.repeat(jnp.exp(heights), dims[dim] // parts).reshape((-1,) + (1,) * (len(dims) - 1 - dim))
    return loudness


def routed_block(stream_key, own, number, rows, number_of, top, most, skew):
    order = jax.random.permutation(stream_key, number_of)
    crowded, usual = portions_of(number_of, rows * top, most, skew, True), portions_of(number_of, rows * top, most, skew, False)
    places = jnp.arange(number_of)

    def named(tallies, rotation):
        used = int((tallies > 0).sum())
        fixed = max(1, used // 4)
        passed = fixed + (places - fixed + rotation * (used - fixed)) % max(1, number_of - fixed)
        return jnp.zeros((number_of,), jnp.int32).at[order[jnp.where(places < fixed, places, passed)]].set(jnp.asarray(tallies, jnp.int32))

    tallies = jnp.where(number % 4 == 0, named(crowded, number // 4), named(usual, number - number // 4 - 1))
    mixed = jax.random.permutation(jax.random.fold_in(own, 3), number_of)
    donor, taker = mixed[0:number_of // 2 * 2:2], mixed[1:number_of // 2 * 2:2]
    margin = jnp.minimum(tallies[donor] - 1, most - tallies[taker]) // 2
    margin = jnp.where((donor == order[0]) | (taker == order[0]) | (tallies[taker] == 0), 0, jnp.maximum(margin, 0))
    passed = jax.random.randint(jax.random.fold_in(own, 4), (number_of // 2,), 0, 1 << 20) % (margin + 1)
    tallies = tallies.at[donor].add(-passed).at[taker].add(passed)
    items = jnp.searchsorted(jnp.cumsum(tallies), jnp.arange(rows * top), side="right").astype(jnp.int32)
    listing = items.reshape(top, rows).T
    listing = listing[jax.random.permutation(jax.random.fold_in(own, 1), rows)]
    rotation = jax.random.randint(jax.random.fold_in(own, 2), (rows, 1), 0, top)
    return jnp.take_along_axis(listing, (jnp.arange(top)[None, :] + rotation) % top, axis=1)


def portions_of(count, total, bound, skew, full):
    loads = [(1 << 20) // math.isqrt(rank ** skew) + 1 for rank in range(1, count + 1)]
    largest = bound if full else min(bound, max(-(-total // count), total * loads[0] // sum(loads)))
    least = 1 if total - largest >= count - 1 else 0
    given, spare = [largest] + [least] * (count - 1), total - largest - least * (count - 1)
    while spare > 0:
        movable = [i for i in range(1, count) if given[i] < largest] or [i for i in range(1, count) if given[i] < bound]
        whole, budget = sum([loads[i] for i in movable]), spare
        for i in movable:
            more = min(bound - given[i], max(1, budget * loads[i] // whole), spare)
            given[i] = given[i] + more
            spare = spare - more
    return np.array(given)


def noise(key, extent, deviation, bound, cuts=(), kind=jnp.bfloat16):
    factor_of = block_levels(key, extent, cuts, -0.22, 0.18) if cuts else 1.0
    array = jax.random.normal(key, extent, jnp.float32) * deviation * factor_of
    return jnp.minimum(jnp.maximum(array, -bound), bound).astype(kind)


def setup_inputs(seed: int = 0) -> dict:
    streams_of = jax.random.split(jax.random.key(seed), 14)
    queries = noise(streams_of[0], (TOKENS1, HEADS * HD), 1.0, 6.0, ((0, 8), (1, 4)))
    key_input = noise(streams_of[1], (TOKENS1, KV_HEADS * HD), 1.0, 6.0, ((0, 8),))
    value_input = noise(streams_of[2], (TOKENS1, KV_HEADS * HD), 1.0, 6.0, ((0, 8),))
    query_gain = jnp.clip(1.0 + 0.18 * jax.random.normal(streams_of[3], (HD,), jnp.float32), 0.1, 1.9)
    key_gain = jnp.clip(1.0 + 0.18 * jax.random.normal(streams_of[4], (HD,), jnp.float32), 0.1, 1.9)
    mix_out_weight = noise(streams_of[5], (HEADS * HD, D), (HEADS * HD) ** -0.5, 0.1875, ((0, 4),))
    expert_input = noise(streams_of[6], (TOKENS2, D), 1.0, 6.0, ((0, 8),))
    ffn_gain = jnp.clip(1.0 + 0.18 * jax.random.normal(streams_of[7], (D,), jnp.float32), 0.1, 1.9)
    routes_keys = jax.random.split(jax.random.fold_in(streams_of[8], 1), TOKENS2 // TOK2)
    routes_turns = jax.random.permutation(jax.random.fold_in(streams_of[8], 3), TOKENS2 // TOK2)
    routes = jax.vmap(lambda own, number: routed_block(jax.random.fold_in(streams_of[8], 2), own, number, TOK2, EXPERTS, TOPK, CAP, 2))(routes_keys, routes_turns).reshape((TOKENS2, TOPK))
    route_scores = jnp.clip(jnp.exp(math.log(1.0) - 2.3025851 * jax.random.uniform(streams_of[9], (TOKENS2, TOPK), jnp.float32) ** block_levels(streams_of[9], (TOKENS2, TOPK), ((0, 8),), -0.2, 0.2)), 0.1, 1.0)
    gate_weight = noise(streams_of[10], (EXPERTS, D, FF), D ** -0.5, 0.125, ((0, 8), (2, 4)))
    up_weight = noise(streams_of[11], (EXPERTS, D, FF), D ** -0.5, 0.125, ((0, 8), (2, 4)))
    down_weight = noise(streams_of[12], (EXPERTS, FF, D), FF ** -0.5, 0.09375, ((0, 8), (1, 4)))
    return dict(queries=queries, key_input=key_input, value_input=value_input, query_gain=query_gain, key_gain=key_gain, mix_out_weight=mix_out_weight, expert_input=expert_input, ffn_gain=ffn_gain, routes=routes, route_scores=route_scores, gate_weight=gate_weight, up_weight=up_weight, down_weight=down_weight)


EPSILON = 1e-06
ROPE_BASE = 10000.0

def rotate_half(portion, cos_table, sin_table):
    front_half, back_half = jnp.split(portion, 2, axis=-1)
    cos_table = cos_table[:, None, :]
    sin_table = sin_table[:, None, :]
    return jnp.concatenate([front_half * cos_table - back_half * sin_table, back_half * cos_table + front_half * sin_table], axis=-1)

def prepare(source, channel_gain, positions):
    token_count = source.shape[0]
    values_f = source.astype(jnp.float32).reshape(token_count, -1, HD)
    normed = values_f * lax.rsqrt(lax.optimization_barrier(jnp.mean(values_f * values_f, axis=-1, keepdims=True)) + EPSILON) * channel_gain
    quarter = HD // 4
    inverse = ROPE_BASE ** (-jnp.arange(quarter, dtype=jnp.float32) / quarter)
    row_angle = (positions // GRID_W).astype(jnp.float32)[:, None] * inverse[None, :]
    col_angle = (positions % GRID_W).astype(jnp.float32)[:, None] * inverse[None, :]
    half_width = HD // 2
    turned = jnp.concatenate([rotate_half(normed[..., :half_width], jnp.cos(row_angle), jnp.sin(row_angle)), rotate_half(normed[..., half_width:], jnp.cos(col_angle), jnp.sin(col_angle))], axis=-1)
    return turned.reshape(token_count, -1).astype(jnp.bfloat16)

def attend_head(head_args):
    query_head, key_head, value_head = head_args
    length = query_head.shape[0]
    key_span = math.gcd(length, 512)
    query_blocks = query_head.reshape(length // key_span, key_span, HD)

    def one_block(query_block):
        scores = jnp.dot(query_block, key_head.T, preferred_element_type=jnp.float32) * HD ** (-0.5)
        weights = jnp.exp(scores)
        weighted = jnp.dot(weights.astype(jnp.bfloat16), value_head, preferred_element_type=jnp.float32)
        return (weighted / lax.optimization_barrier(jnp.sum(weights, axis=-1, keepdims=True))).astype(jnp.bfloat16)
    return lax.map(one_block, query_blocks).reshape(length, HD)

def reference(queries, key_input, value_input, query_gain, key_gain, mix_out_weight, expert_input, ffn_gain, routes, route_scores, gate_weight, up_weight, down_weight):
    length = queries.shape[0]
    positions = jnp.arange(length, dtype=jnp.int32)
    group_size = HEADS // KV_HEADS
    q_rot = prepare(queries, query_gain, positions).reshape(length, HEADS, HD).transpose(1, 0, 2)
    k_rot = prepare(key_input, key_gain, positions).reshape(length, KV_HEADS, HD).transpose(1, 0, 2)
    v_heads = value_input.reshape(length, KV_HEADS, HD).transpose(1, 0, 2)
    attended = lax.map(attend_head, (q_rot, jnp.repeat(k_rot, group_size, axis=0), jnp.repeat(v_heads, group_size, axis=0)))
    attended = attended.transpose(1, 0, 2).reshape(length, HEADS * HD)
    col_width = HEADS * HD // N_TP

    def add_group(running_sum, group_index):
        start_col = (group_index * col_width).astype(jnp.int32)
        columns = lax.dynamic_slice_in_dim(attended, start_col, col_width, 1)
        weight_rows = lax.dynamic_slice_in_dim(mix_out_weight, start_col, col_width, 0)
        portion = jnp.dot(columns, weight_rows, preferred_element_type=jnp.float32).astype(jnp.bfloat16)
        portion = lax.optimization_barrier(portion)
        return (running_sum + portion.astype(jnp.float32), None)
    mixed_sum, _ = lax.scan(add_group, jnp.zeros((length, D), jnp.float32), jnp.arange(N_TP, dtype=jnp.int32))
    mixed_rows = mixed_sum.astype(jnp.bfloat16)
    tokens = expert_input.shape[0]
    flat_routes = routes.reshape(N_EP, TOK2 * TOPK)
    hit_table = (flat_routes[:, :, None] == jnp.arange(EXPERTS, dtype=jnp.int32)[None, None, :]).astype(jnp.int32)
    position = lax.optimization_barrier(jnp.sum((jnp.cumsum(hit_table, axis=1) - hit_table) * hit_table, axis=-1))
    per_expert = N_EP * CAP
    slot_index = flat_routes * per_expert + jnp.arange(N_EP, dtype=jnp.int32)[:, None] * CAP + position
    slot_index = slot_index.reshape(-1).astype(jnp.int32)
    pair_token = jnp.arange(tokens * TOPK, dtype=jnp.int32) // TOPK
    owner_row = jnp.full((EXPERTS * per_expert,), tokens, jnp.int32).at[slot_index].set(pair_token)
    padded = jnp.concatenate([expert_input, jnp.zeros((1, D), jnp.bfloat16)], axis=0)
    buffers = padded[owner_row].reshape(EXPERTS, per_expert, D)
    ff_width = FF // N_TP

    def run_expert(expert_args):
        slot_rows, w_gate, w_up, w_down = expert_args
        values_f = slot_rows.astype(jnp.float32)
        row_scale = lax.rsqrt(lax.optimization_barrier(jnp.mean(values_f * values_f, axis=-1, keepdims=True)) + EPSILON)
        scaled = (values_f * ffn_gain).astype(jnp.bfloat16)
        gate_pre = row_scale * jnp.dot(scaled, w_gate, preferred_element_type=jnp.float32)
        up_pre = row_scale * jnp.dot(scaled, w_up, preferred_element_type=jnp.float32)
        hidden = (jax.nn.silu(gate_pre) * up_pre).astype(jnp.bfloat16)
        running_sum = jnp.zeros((per_expert, D), jnp.float32)
        for group_index in range(N_TP):
            lower = group_index * ff_width
            portion = jnp.dot(hidden[:, lower:lower + ff_width], w_down[lower:lower + ff_width], preferred_element_type=jnp.float32).astype(jnp.bfloat16)
            running_sum = running_sum + lax.optimization_barrier(portion).astype(jnp.float32)
        return running_sum.astype(jnp.bfloat16)
    pair_rows = lax.map(run_expert, (buffers, gate_weight, up_weight, down_weight)).reshape(-1, D)
    route_weight = route_scores / lax.optimization_barrier(jnp.sum(route_scores, axis=-1, keepdims=True))
    picked = pair_rows[slot_index].astype(jnp.float32).reshape(tokens, TOPK, D)
    expert_out = lax.optimization_barrier(jnp.sum(picked * route_weight[:, :, None], axis=1)).astype(jnp.bfloat16)
    return (mixed_rows, expert_out)
```

```python
import functools
import math

import jax
import jax.numpy as jnp
from jax import lax
from jax.experimental import pallas as pl
from jax.experimental.pallas import tpu as pltpu
from jax.sharding import PartitionSpec as P

HEADS = 16
KV_HEADS = 4
HD = 64
GRID_W = 64
EPSILON = 1e-06
ROPE_BASE = 10000.0
MESH = pl.DeviceIdType.MESH
LANES = 128
BF = jnp.bfloat16
F32 = jnp.float32


def prep(values, gain, cos_table, sin_table):
    width = values.shape[1]
    squares = values * values
    high = squares.astype(BF)
    low = (squares - high.astype(F32)).astype(BF)
    rows = lax.broadcasted_iota(jnp.int32, (width, width), 0) // HD
    cols = lax.broadcasted_iota(jnp.int32, (width, width), 1) // HD
    same = jnp.where(rows == cols, 1.0, 0.0).astype(BF)
    total = jnp.dot(high, same, preferred_element_type=F32) + jnp.dot(
        low, same, preferred_element_type=F32
    )
    gain = jnp.concatenate([gain] * (width // HD), axis=1)
    normed = values * lax.rsqrt(total * (1.0 / HD) + EPSILON) * gain
    lane = lax.broadcasted_iota(jnp.int32, normed.shape, 1)
    quarter = HD // 4
    partner = jnp.where(
        lane % (2 * quarter) < quarter,
        pltpu.roll(normed, width - quarter, 1),
        pltpu.roll(normed, quarter, 1),
    )
    return normed * cos_table + partner * sin_table


def angle_tables(start, rows):
    quarter = HD // 4
    many = rows // GRID_W

    def both(count, first):
        shape = (count, LANES)
        place = lax.broadcasted_iota(jnp.int32, shape, 0) + first
        lane = lax.broadcasted_iota(jnp.int32, shape, 1)
        turn = lane % quarter
        inverse = jnp.zeros(shape, F32)
        for j in range(quarter):
            inverse = jnp.where(turn == j, ROPE_BASE ** (-j / quarter), inverse)
        angle = place.astype(F32) * inverse
        sign = jnp.where(lane % (2 * quarter) < quarter, -1.0, 1.0)
        return jnp.cos(angle), jnp.sin(angle) * sign

    tables = []
    for by_row, by_col in zip(both(max(many, 8), start // GRID_W), both(GRID_W, 0)):
        lane = lax.broadcasted_iota(jnp.int32, by_col.shape, 1)
        tables.append(
            jnp.concatenate(
                [jnp.where(lane % HD < HD // 2, by_row[i:i + 1, :], by_col) for i in range(many)],
                axis=0,
            )
        )
    return tables


def mark(name):
    pass


def kernel(
    n_ep, n_tp, heads, model_width,
    q_any, k_any, v_any, qg_any, kg_any, wmix_any, x_any, gain_any, routes_any, scores_any, wg_any, wu_any, wd_any,
    mixed_ref, out_ref,
    q_ref, k_in, v_in, x_ref, qg_ref, kg_ref, gain_ref, routes_ref, scores_ref, wg, wu, wd, wmix,
    kv_buf, q_buf, acc, x_out, x_buf, scaled, hid, dp_buf, ep_in, es_buf, ey_in,
    ret_out, ret_in, mp_out, mp_in, ms_out, my_in,
    w_sem, kvx_s, kvz_s, kv_r, di_s, di_r, dy_s, dy_r, dc_s, dc_r, ep_s, ep_r, ey_s, ey_r, rt_s, rt_r,
    mp_s, mp_r, my_s, my_r,
):
    n_y = n_tp // 2
    n_x = 1 << ((n_ep.bit_length() - 1) // 2)
    n_z = n_ep // n_x
    stages = n_z - 1
    me = lax.axis_index("ep")
    tp = lax.axis_index("tp")
    my_y, core = tp // 2, tp % 2
    my_z, my_x = me // n_x, me % n_x
    mate = my_y * 2 + 1 - core
    rows = q_ref.shape[0]
    kv_head = tp * heads // (HEADS // KV_HEADS)
    kv_tile = pl.ds(pl.multiple_of(kv_head // 2 * LANES, LANES), LANES)
    slots_per, col_w = x_buf.shape[2:]
    slots = n_ep * slots_per
    group = n_x * slots_per
    tokens = x_ref.shape[0]
    x_cols = pl.ds(pl.multiple_of(tp * col_w, col_w), col_w)

    def y_peer(j):
        return (my_y + j) % n_y

    def z_other(o):
        z = my_z
        for bit in range(n_z.bit_length() - 1):
            if o >> bit & 1:
                z = z + (1 - 2 * (my_z // (1 << bit) % 2)) * (1 << bit)
        return z

    def ep_other(o, i):
        return z_other(o) * n_x + (my_x + i) % n_x

    mark("a_greet")
    barrier = pltpu.get_barrier_semaphore()

    def greet(o, carry):
        pl.semaphore_signal(barrier, inc=1, device_id=((me + o) % n_ep, tp), device_id_type=MESH)
        return carry

    lax.fori_loop(1, n_ep, greet, 0)
    for j in range(1, n_y):
        pl.semaphore_signal(
            barrier, inc=1, device_id=(me, y_peer(j) * 2 + core), device_id_type=MESH
        )
    pl.semaphore_signal(barrier, inc=1, device_id=(me, mate), device_id_type=MESH)

    loads = [
        pltpu.make_async_copy(src, dst, w_sem.at[i])
        for i, (src, dst) in enumerate(
            (
                (routes_any, routes_ref),
                (x_any.at[:, x_cols], x_ref),
                (kg_any, kg_ref),
                (k_any.at[:, kv_tile], k_in),
                (v_any.at[:, kv_tile], v_in),
                (qg_any, qg_ref),
                (q_any, q_ref),
                (gain_any, gain_ref),
                (scores_any, scores_ref),
                (wg_any.at[0], wg),
                (wu_any.at[0], wu),
                (wd_any.at[0], wd),
                (wmix_any, wmix),
            )
        )
    ]
    for load in loads:
        load.start()

    mark("b_route")
    loads[0].wait()
    expert_row = lax.broadcasted_iota(jnp.int32, (n_ep, tokens), 0)
    first = jnp.where(expert_row == routes_ref[0:1, :], 1.0, 0.0)
    second = jnp.where(expert_row == routes_ref[1:2, :], 1.0, 0.0)
    earlier = jnp.where(
        lax.broadcasted_iota(jnp.int32, (tokens, tokens), 0)
        < lax.broadcasted_iota(jnp.int32, (tokens, tokens), 1),
        1.0,
        0.0,
    ).astype(BF)
    before = jnp.dot((first + second).astype(BF), earlier, preferred_element_type=F32)
    place = before + expert_row.astype(F32) * slots_per
    slot_a = jnp.sum(first * place, axis=0, keepdims=True).astype(jnp.int32)
    slot_b = jnp.sum(second * place, axis=0, keepdims=True).astype(jnp.int32)
    slot_row = lax.broadcasted_iota(jnp.int32, (slots, tokens), 0)
    pick_a = jnp.where(slot_row == slot_a, 1.0, 0.0).astype(BF)
    pick_b = jnp.where(slot_row == slot_b, 1.0, 0.0).astype(BF)
    mark("c_pack")
    loads[1].wait()
    sent = jnp.dot(pick_a + pick_b, x_ref[...], preferred_element_type=F32).astype(BF)
    x_out[...] = sent.reshape(x_out.shape)
    x_buf[tp, me] = x_out[me]

    mark("d_barrier")
    pl.semaphore_wait(barrier, n_ep - 1 + n_y)

    def disp(peer, source):
        return pltpu.make_async_remote_copy(
            x_out.at[peer], x_buf.at[tp, source], di_s.at[peer], di_r.at[source],
            device_id=(peer, tp), device_id_type=MESH,
        )

    def over_y(j, source, owner):
        return pltpu.make_async_remote_copy(
            x_buf.at[owner * 2 + core, source], x_buf.at[owner * 2 + core, source],
            dy_s.at[y_peer(j), source], dy_r.at[owner, source],
            device_id=(me, y_peer(j) * 2 + core), device_id_type=MESH,
        )

    mark("e_disp")
    for o in range(n_z):

        def start_disp(i, carry):
            disp(ep_other(o, i), me).start()
            return carry

        lax.fori_loop(1 if o == 0 else 0, n_x, start_disp, 0)
    for j in range(1, n_y):
        over_y(j, me, my_y).start()

    def x_peer(i):
        return my_z * n_x + (my_x + i) % n_x

    def kv_send(peer, origin, sem):
        return pltpu.make_async_remote_copy(
            kv_buf.at[origin], kv_buf.at[origin], sem, kv_r.at[origin],
            device_id=(peer, tp), device_id_type=MESH,
        )

    mark("f_prepk")
    cos_table, sin_table = angle_tables(me * rows, rows)
    for i in (2, 3, 4):
        loads[i].wait()
    odd = kv_head % 2 == 1
    key = k_in[...].astype(F32)
    value = v_in[...].astype(F32)
    key = jnp.where(odd, pltpu.roll(key, HD, 1), key)
    value = jnp.where(odd, value, pltpu.roll(value, HD, 1))
    turned = prep(key, kg_ref[...], cos_table, sin_table)
    lane = lax.broadcasted_iota(jnp.int32, key.shape, 1)
    kv_buf[me] = jnp.where(lane < HD, turned, value).astype(BF)

    def own_kv_right():
        return kv_send((my_z + 1) % n_z * n_x + my_x, me, kvz_s.at[my_z, 0])

    def own_kv_left():
        return kv_send((my_z + n_z - 1) % n_z * n_x + my_x, me, kvz_s.at[my_z, 1])

    for i in range(1, n_x):
        kv_send(x_peer(i), me, kvx_s.at[my_z, i]).start()

    @pl.when(my_z < n_z - 1)
    def _():
        own_kv_right().start()

    @pl.when(my_z > 0)
    def _():
        own_kv_left().start()

    side = my_z // (n_z // 2)
    outward = 1 - 2 * side
    inner = my_z + side * (n_z - 1 - 2 * my_z)

    def z_near(k):
        step = jnp.where(
            k <= 2 * inner, (k + 1) // 2 * (-1 if k % 2 else 1), k - inner
        )
        return my_z + outward * step

    def kv_onward(k):
        z = z_near(k)
        onward = my_z + jnp.where(z < my_z, 1, -1)
        inside = jnp.logical_and(onward >= 0, onward < n_z)
        peer = (onward + n_z) % n_z * n_x + my_x
        return inside, kv_send(peer, z * n_x + my_x, kvz_s.at[z, 0])

    def kv_forward(k):
        z = z_near(k)
        origin = z * n_x + my_x
        kv_send(origin, origin, kvz_s.at[z, 0]).wait_recv()
        inside, onward = kv_onward(k)

        @pl.when(inside)
        def _():
            onward.start()

        for i in range(1, n_x):
            kv_send(x_peer(i), origin, kvx_s.at[z, i]).start()

    mark("f_prepq")
    factor = HD ** (-0.5) * math.log2(math.e)
    loads[5].wait()
    loads[6].wait()
    for tile in range(q_ref.shape[1] // LANES):
        q_tile = factor * prep(
            q_ref[:, tile * LANES:(tile + 1) * LANES].astype(F32),
            qg_ref[...], cos_table, sin_table,
        )
        q_lane = lax.broadcasted_iota(jnp.int32, q_tile.shape, 1)
        for part in range(2):
            head = tile * 2 + part
            if head < heads:
                moved = q_tile if part == 0 else pltpu.roll(q_tile, HD, 1)
                q_buf[head] = jnp.where(q_lane < HD, moved, 0.0).astype(BF)

    piece = rows // n_y
    half = piece // 2

    def attend(block, owner, fresh=False):
        start = pl.multiple_of(owner * piece, piece)
        q_rows = q_buf[:, pl.ds(start, piece), :].reshape(heads * piece, LANES)
        kv = kv_buf[block]
        logits = lax.dot_general(
            q_rows, kv, (((1,), (1,)), ((), ())), preferred_element_type=F32
        )
        weights = jnp.exp2(logits).astype(BF)
        kv_lane = lax.broadcasted_iota(jnp.int32, kv.shape, 1)
        values = jnp.where(kv_lane < HD, jnp.ones_like(kv), kv)
        part = jnp.dot(weights, values, preferred_element_type=F32)
        acc[owner] = part if fresh else acc[owner] + part

    def attend_all(block, fresh=False):
        def one(owner, carry):
            attend(block, owner, fresh)
            return carry

        lax.fori_loop(0, n_y, one, 0)

    def kv_arrived(origin):
        kv_send(origin, origin, kvx_s.at[0, 0]).wait_recv()

    def others_attend(z):
        def one(i, carry):
            origin = z * n_x + (my_x + i) % n_x
            kv_arrived(origin)
            attend_all(origin)
            return carry

        lax.fori_loop(1, n_x, one, 0)

    def base(s):
        return my_z // 2 * 2 if s == 0 else z_other(s + 1)

    def many(s):
        return 2 if s == 0 else 1

    def members(s):
        return pl.ds(base(s) * n_x, many(s) * n_x)

    def stage_rows(s):
        return pl.ds(pl.multiple_of(base(s) * group, group), many(s) * group)

    def to_mate(owner, mine, s):
        part = x_buf.at[owner * 2 + mine, members(s)]
        return pltpu.make_async_remote_copy(
            part, part, dc_s.at[owner, s], dc_r.at[owner, s],
            device_id=(me, mate), device_id_type=MESH,
        )

    def pass_on(s):
        for o in (0, 1) if s == 0 else (s + 1,):

            def one(i, carry):
                source = ep_other(o, i)
                disp(source, source).wait_recv()
                for j in range(1, n_y):
                    over_y(j, source, my_y).start()
                return carry

            lax.fori_loop(1 if o == 0 else 0, n_x, one, 0)
        to_mate(my_y, core, s).start()

    def from_y(s):
        for j in range(1, n_y):
            owner = y_peer(j)

            def arrived(i, carry):
                over_y(j, base(s) * n_x + i, owner).wait_recv()
                return carry

            lax.fori_loop(0, many(s) * n_x, arrived, 0)
            to_mate(owner, core, s).start()

    def expert_in(s):
        for j in range(n_y):
            to_mate(y_peer(j), 1 - core, s).wait_recv()
        count = many(s) * group
        power = jnp.zeros((count, 1), F32)
        for q in range(n_tp):
            x_q = x_buf[q, members(s)].reshape(count, col_w).astype(F32)
            power = power + jnp.sum(x_q * x_q, axis=1, keepdims=True)
            scaled[stage_rows(s), q * col_w:(q + 1) * col_w] = (
                x_q * gain_ref[:, q * col_w:(q + 1) * col_w]
            ).astype(BF)
        return lax.rsqrt(power * (1.0 / model_width) + EPSILON)

    hidden_w = wg.shape[1]
    tile_w = math.gcd(hidden_w, 512)

    def expert_hidden(s, row_scale):
        at = stage_rows(s)

        def hidden_tile(i, carry):
            cols = pl.ds(pl.multiple_of(i * tile_w, tile_w), tile_w)
            gate = row_scale * jnp.dot(scaled[at, :], wg[:, cols], preferred_element_type=F32)
            up = row_scale * jnp.dot(scaled[at, :], wu[:, cols], preferred_element_type=F32)
            hid[at, cols] = (gate / (1.0 + jnp.exp(-gate)) * up).astype(BF)
            return carry

        lax.fori_loop(0, hidden_w // tile_w, hidden_tile, 0)

    def expert_mate(owner, side, s):
        return pltpu.make_async_remote_copy(
            dp_buf.at[owner * 2 + side, stage_rows(s)], ep_in.at[owner, stage_rows(s)],
            ep_s.at[owner, s], ep_r.at[owner, s],
            device_id=(me, mate), device_id_type=MESH,
        )

    def expert_y(j, origin, s):
        return pltpu.make_async_remote_copy(
            es_buf.at[y_peer(j), stage_rows(s)], ey_in.at[origin, stage_rows(s)],
            ey_s.at[y_peer(j), s], ey_r.at[origin, s],
            device_id=(me, y_peer(j) * 2 + core), device_id_type=MESH,
        )

    def expert_down(s):
        at = stage_rows(s)
        for whose in (1 - core, core):
            for j in range(1, n_y + 1):
                owner = y_peer(j)
                q = owner * 2 + whose
                cols = pl.ds(pl.multiple_of(q * col_w, col_w), col_w)
                dp_buf[q, at] = jnp.dot(
                    hid[at, :], wd[:, cols], preferred_element_type=F32
                ).astype(BF)
                if whose is not core:
                    expert_mate(owner, 1 - core, s).start()

    def mate_sum(j, s):
        owner = y_peer(j)
        expert_mate(owner, core, s).wait_recv()
        at = stage_rows(s)
        return dp_buf[owner * 2 + core, at].astype(F32) + ep_in[owner, at].astype(F32)

    def expert_send(s):
        for j in range(1, n_y):
            es_buf[y_peer(j), stage_rows(s)] = mate_sum(j, s).astype(BF)
            expert_y(j, my_y, s).start()

    def ret(peer, origin):
        return pltpu.make_async_remote_copy(
            ret_out.at[peer], ret_in.at[origin], rt_s.at[peer], rt_r.at[origin],
            device_id=(peer, tp), device_id_type=MESH,
        )

    def expert_return(s):
        total = mate_sum(0, s)
        for j in range(1, n_y):
            expert_y(j, y_peer(j), s).wait_recv()
            total = total + ey_in[y_peer(j), stage_rows(s)].astype(F32)
        ret_out[members(s)] = total.astype(BF).reshape(many(s) * n_x, slots_per, col_w)
        for o in (0, 1) if s == 0 else (s + 1,):

            def one(i, carry):
                ret(ep_other(o, i), me).start()
                return carry

            lax.fori_loop(1 if o == 0 else 0, n_x, one, 0)
        if s == 0:
            ret_in[me] = ret_out[me]

    def mix_mate(owner, side):
        return pltpu.make_async_remote_copy(
            mp_out.at[owner, side], mp_in.at[owner], mp_s.at[owner], mp_r.at[owner],
            device_id=(me, mate), device_id_type=MESH,
        )

    def mix_y(j, origin):
        return pltpu.make_async_remote_copy(
            ms_out.at[y_peer(j)], my_in.at[origin], my_s.at[y_peer(j)], my_r.at[origin],
            device_id=(me, y_peer(j) * 2 + core), device_id_type=MESH,
        )

    def mix(owner):
        total = acc[owner]
        ratio = (total / pltpu.roll(total, HD, 1)).reshape(heads, piece, LANES)
        out_lane = lax.broadcasted_iota(jnp.int32, (piece, LANES), 1)
        tiles = []
        for tile in range(q_ref.shape[1] // LANES):
            left = pltpu.roll(ratio[2 * tile], HD, 1)
            right = ratio[2 * tile + 1] if 2 * tile + 1 < heads else jnp.zeros_like(left)
            tiles.append(jnp.where(out_lane < HD, left, right).astype(BF))
        attended = tiles[0] if len(tiles) == 1 else jnp.concatenate(tiles, axis=1)
        part = jnp.dot(attended, wmix[...], preferred_element_type=F32).astype(BF)
        mp_out[owner] = part.reshape(2, half, part.shape[1])
        mix_mate(owner, 1 - core).start()

    def mix_sum(owner):
        mix_mate(owner, core).wait_recv()
        return mp_out[owner, core].astype(F32) + mp_in[owner].astype(F32)

    mark("g_pass0")
    pass_on(0)
    mark("g_attown")
    attend_all(me, True)
    mark("g_attownx")
    others_attend(my_z)
    mark("g_kvf1")
    kv_forward(1)
    mark("g_fromy0")
    from_y(0)
    mark("g_att1")
    attend_all(z_near(1) * n_x + my_x)
    mark("h_in0")
    loads[7].wait()
    row_scale = expert_in(0)
    mark("h_hid0")
    loads[9].wait()
    loads[10].wait()
    expert_hidden(0, row_scale)
    mark("h_pass1")
    if stages > 1:
        pass_on(1)
    mark("h_down0")
    loads[11].wait()
    expert_down(0)
    mark("h_kvf2")
    if n_z > 2:
        kv_forward(2)
    mark("h_att1x")
    others_attend(z_near(1))
    mark("h_send0")
    expert_send(0)
    for s in range(1, stages):
        mark(f"i_fromy{s}")
        from_y(s)
        mark(f"i_kvf{s+2}")
        if s + 2 < n_z:
            kv_forward(s + 2)
        mark(f"i_in{s}")
        row_scale = expert_in(s)
        mark(f"i_hid{s}")
        expert_hidden(s, row_scale)
        mark(f"i_pass{s+1}")
        if s + 1 < stages:
            pass_on(s + 1)
        mark(f"i_down{s}")
        expert_down(s)
        mark(f"i_ret{s-1}")
        expert_return(s - 1)
        mark(f"i_send{s}")
        expert_send(s)

    mark("j_farkv")

    def far_attend(owner):
        for k in range(2, n_z):
            z = z_near(k)

            def one(i, carry):
                attend(z * n_x + (my_x + i) % n_x, owner)
                return carry

            lax.fori_loop(0, n_x, one, 0)

    for k in range(2, n_z):
        for i in range(1, n_x):
            kv_arrived(z_near(k) * n_x + (my_x + i) % n_x)
    mark("j_loadmix")
    loads[12].wait()
    for j in range(1, n_y):
        mark("j_att")
        far_attend(y_peer(j))
        if j == 1:
            mark("j_ret")
            expert_return(stages - 1)
        mark("j_mix")
        mix(y_peer(j))
    mark("k_att")
    far_attend(my_y)
    for j in range(1, n_y):
        mark("k_mixsum")
        ms_out[y_peer(j)] = mix_sum(y_peer(j)).astype(BF)
        mix_y(j, my_y).start()
    mark("k_mix")
    mix(my_y)

    mark("l_retwait")

    def ret_wait(o, carry):
        source = (me + n_ep - o) % n_ep
        ret(source, source).wait_recv()
        return carry

    lax.fori_loop(1, n_ep, ret_wait, 0)
    mark("m_combine")
    loads[8].wait()
    back = ret_in[...].reshape(slots, col_w)
    share_row = scores_ref[...] / jnp.sum(scores_ref[...], axis=0, keepdims=True)
    own_token = lax.broadcasted_iota(jnp.int32, (tokens, tokens), 0) == lax.broadcasted_iota(
        jnp.int32, (tokens, tokens), 1
    )
    share_a, share_b = (
        jnp.sum(jnp.where(own_token, share_row[i:i + 1, :], 0.0), axis=1, keepdims=True)
        for i in range(2)
    )
    rows_a = lax.dot_general(
        pick_a, back, (((0,), (0,)), ((), ())), preferred_element_type=F32
    )
    rows_b = lax.dot_general(
        pick_b, back, (((0,), (0,)), ((), ())), preferred_element_type=F32
    )
    out_ref[...] = (rows_a * share_a + rows_b * share_b).astype(BF)

    mark("n_mixsum")
    total = mix_sum(my_y)
    mark("n_ywait")
    for j in range(1, n_y):
        mix_y(j, y_peer(j)).wait_recv()
        total = total + my_in[y_peer(j)].astype(F32)
    mark("n_out")
    mixed_ref[...] = total.astype(BF)

    mark("o_sends")

    def sends(o, carry):
        peer = (me + o) % n_ep
        disp(peer, me).wait_send()
        ret(peer, me).wait_send()
        return carry

    lax.fori_loop(1, n_ep, sends, 0)
    for i in range(1, n_x):

        def sent_x(z, carry):
            kv_send(x_peer(i), z * n_x + my_x, kvx_s.at[z, i]).wait_send()
            return carry

        lax.fori_loop(0, n_z, sent_x, 0)

    @pl.when(my_z < n_z - 1)
    def _():
        own_kv_right().wait_send()

    @pl.when(my_z > 0)
    def _():
        own_kv_left().wait_send()

    for k in range(1, n_z):
        inside, onward = kv_onward(k)

        @pl.when(inside)
        def _():
            onward.wait_send()

    for j in range(1, n_y):

        def sent_y(source, carry):
            over_y(j, source, my_y).wait_send()
            return carry

        lax.fori_loop(0, n_ep, sent_y, 0)
        mix_y(j, my_y).wait_send()
    for j in range(n_y):
        for s in range(stages):
            to_mate(y_peer(j), core, s).wait_send()
            expert_mate(y_peer(j), 1 - core, s).wait_send()
            if j:
                expert_y(j, my_y, s).wait_send()
        mix_mate(y_peer(j), 1 - core).wait_send()
    mark(None)


def local(
    n_ep, n_tp,
    queries, key_input, value_input, query_gain, key_gain, mix_out_weight, expert_input, ffn_gain,
    routes, route_scores, gate_weight, up_weight, down_weight,
):
    rows = queries.shape[0]
    heads = queries.shape[1] // HD
    n_y = n_tp // 2
    n_x = 1 << ((n_ep.bit_length() - 1) // 2)
    n_z = n_ep // n_x
    stages = n_z - 1
    spare = heads % 2 * HD
    if spare:
        queries = jnp.pad(queries, ((0, 0), (0, spare)))
        mix_out_weight = jnp.pad(mix_out_weight, ((0, spare), (0, 0)))
    width = expert_input.shape[1]
    col_w = width // n_tp
    tokens, top = routes.shape
    capacity = 3 * tokens * top // (2 * n_ep)
    slots_per = -(-capacity // 16) * 16
    slots = n_ep * slots_per
    hidden_w = gate_weight.shape[2]
    out_w = mix_out_weight.shape[1]
    half = rows // n_tp
    vm = pltpu.VMEM
    dma = pltpu.SemaphoreType.DMA
    scratch = [
        vm(queries.shape, BF), vm((rows, LANES), BF), vm((rows, LANES), BF), vm((tokens, col_w), BF),
        vm((1, HD), F32), vm((1, HD), F32), vm((1, width), F32), vm((top, tokens), jnp.int32), vm((top, tokens), F32),
        vm((width, hidden_w), BF), vm((width, hidden_w), BF), vm((hidden_w, width), BF),
        vm(mix_out_weight.shape, BF),
        vm((n_ep, rows, LANES), BF), vm((heads, rows, LANES), BF), vm((n_y, heads * rows // n_y, LANES), F32),
        vm((n_ep, slots_per, col_w), BF), vm((n_tp, n_ep, slots_per, col_w), BF),
        vm((slots, width), BF), vm((slots, hidden_w), BF),
        vm((n_tp, slots, col_w), BF), vm((n_y, slots, col_w), BF), vm((n_y, slots, col_w), BF),
        vm((n_y, slots, col_w), BF),
        vm((n_ep, slots_per, col_w), BF), vm((n_ep, slots_per, col_w), BF),
        vm((n_y, 2, half, out_w), BF), vm((n_y, half, out_w), BF), vm((n_y, half, out_w), BF),
        vm((n_y, half, out_w), BF),
        dma((13,)),
        dma((n_z, n_x)), dma((n_z, 2)), dma((n_ep,)), dma((n_ep,)), dma((n_ep,)),
        dma((n_y, n_ep)), dma((n_y, n_ep)),
    ] + [dma((n_y, stages))] * 6 + [dma((n_ep,))] * 2 + [dma((n_y,))] * 4
    in_vmem = pl.BlockSpec(memory_space=pltpu.VMEM)
    in_hbm = pl.BlockSpec(memory_space=pltpu.HBM)
    return pl.pallas_call(
        functools.partial(kernel, n_ep, n_tp, heads, width),
        out_shape=(
            jax.ShapeDtypeStruct((half, out_w), BF),
            jax.ShapeDtypeStruct((tokens, col_w), BF),
        ),
        in_specs=[in_hbm] * 13,
        out_specs=(in_vmem, in_vmem),
        scratch_shapes=scratch,
        compiler_params=pltpu.CompilerParams(
            collective_id=0, has_side_effects=True, vmem_limit_bytes=60 * 1024 * 1024
        ),
    )(
        queries, key_input, value_input, query_gain[None, :], key_gain[None, :],
        mix_out_weight, expert_input, ffn_gain[None, :], routes.T, route_scores.T,
        gate_weight, up_weight, down_weight,
    )


def solution(mesh):
    placed = (
        P("ep", "tp"),
        P("ep", None),
        P("ep", None),
        P(),
        P(),
        P("tp", None),
        P("ep", None),
        P(),
        P("ep", None),
        P("ep", None),
        P("ep", None, "tp"),
        P("ep", None, "tp"),
        P("ep", "tp", None),
    )
    return jax.shard_map(
        functools.partial(local, mesh.shape["ep"], mesh.shape["tp"]),
        mesh=mesh,
        in_specs=placed,
        out_specs=(P(("ep", "tp"), None), P("ep", "tp")),
        check_vma=False,
    )
```

```python
import functools
import math

import jax
import jax.numpy as jnp
from jax import lax
from jax.experimental import pallas as pl
from jax.experimental.pallas import tpu as pltpu
from jax.sharding import PartitionSpec as P

HEADS = 16
KV_HEADS = 4
HD = 64
GRID_W = 64
EPSILON = 1e-06
ROPE_BASE = 10000.0
MESH = pl.DeviceIdType.MESH
LANES = 128
BF = jnp.bfloat16
F32 = jnp.float32


def prep(values, gain, cos_table, sin_table):
    width = values.shape[1]
    squares = values * values
    high = squares.astype(BF)
    low = (squares - high.astype(F32)).astype(BF)
    rows = lax.broadcasted_iota(jnp.int32, (width, width), 0) // HD
    cols = lax.broadcasted_iota(jnp.int32, (width, width), 1) // HD
    same = jnp.where(rows == cols, 1.0, 0.0).astype(BF)
    total = jnp.dot(high, same, preferred_element_type=F32) + jnp.dot(
        low, same, preferred_element_type=F32
    )
    gain = jnp.concatenate([gain] * (width // HD), axis=1)
    normed = values * lax.rsqrt(total * (1.0 / HD) + EPSILON) * gain
    lane = lax.broadcasted_iota(jnp.int32, normed.shape, 1)
    quarter = HD // 4
    partner = jnp.where(
        lane % (2 * quarter) < quarter,
        pltpu.roll(normed, width - quarter, 1),
        pltpu.roll(normed, quarter, 1),
    )
    return normed * cos_table + partner * sin_table


def angle_tables(start, rows):
    quarter = HD // 4
    many = rows // GRID_W

    def both(count, first):
        shape = (count, LANES)
        place = lax.broadcasted_iota(jnp.int32, shape, 0) + first
        lane = lax.broadcasted_iota(jnp.int32, shape, 1)
        turn = lane % quarter
        inverse = jnp.zeros(shape, F32)
        for j in range(quarter):
            inverse = jnp.where(turn == j, ROPE_BASE ** (-j / quarter), inverse)
        angle = place.astype(F32) * inverse
        sign = jnp.where(lane % (2 * quarter) < quarter, -1.0, 1.0)
        return jnp.cos(angle), jnp.sin(angle) * sign

    tables = []
    for by_row, by_col in zip(both(max(many, 8), start // GRID_W), both(GRID_W, 0)):
        lane = lax.broadcasted_iota(jnp.int32, by_col.shape, 1)
        tables.append(
            jnp.concatenate(
                [jnp.where(lane % HD < HD // 2, by_row[i:i + 1, :], by_col) for i in range(many)],
                axis=0,
            )
        )
    return tables


def mark(name):
    pass


def kernel(
    n_ep, n_tp, heads, model_width,
    q_any, k_any, v_any, qg_any, kg_any, wmix_any, x_any, gain_any, routes_any, scores_any, wg_any, wu_any, wd_any,
    mixed_ref, out_ref,
    q_ref, k_in, v_in, x_ref, qg_ref, kg_ref, gain_ref, routes_ref, scores_ref, wg, wu, wd, wmix,
    kv_buf, q_buf, acc, x_out, x_buf, scaled, hid, dp_buf, ep_in, es_buf, ey_in,
    ret_out, ret_in, mp_out, mp_in, ms_out, my_in,
    w_sem, kvx_s, kvz_s, kv_r, di_s, di_r, dy_s, dy_r, dc_s, dc_r, ep_s, ep_r, ey_s, ey_r, rt_s, rt_r,
    mp_s, mp_r, my_s, my_r,
):
    n_y = n_tp // 2
    n_x = 1 << ((n_ep.bit_length() - 1) // 2)
    n_z = n_ep // n_x
    stages = n_z
    me = lax.axis_index("ep")
    tp = lax.axis_index("tp")
    my_y, core = tp // 2, tp % 2
    my_z, my_x = me // n_x, me % n_x
    mate = my_y * 2 + 1 - core
    rows = q_ref.shape[0]
    kv_head = tp * heads // (HEADS // KV_HEADS)
    kv_tile = pl.ds(pl.multiple_of(kv_head // 2 * LANES, LANES), LANES)
    slots_per, col_w = x_buf.shape[2:]
    slots = n_ep * slots_per
    group = n_x * slots_per
    tokens = x_ref.shape[0]
    x_cols = pl.ds(pl.multiple_of(tp * col_w, col_w), col_w)

    def y_peer(j):
        return (my_y + j) % n_y

    def z_other(o):
        z = my_z
        for bit in range(n_z.bit_length() - 1):
            if o >> bit & 1:
                z = z + (1 - 2 * (my_z // (1 << bit) % 2)) * (1 << bit)
        return z

    def ep_other(o, i):
        return z_other(o) * n_x + (my_x + i) % n_x

    loads = [
        pltpu.make_async_copy(src, dst, w_sem.at[i])
        for i, (src, dst) in enumerate(
            (
                (routes_any, routes_ref),
                (x_any.at[:, x_cols], x_ref),
                (kg_any, kg_ref),
                (k_any.at[:, kv_tile], k_in),
                (v_any.at[:, kv_tile], v_in),
                (qg_any, qg_ref),
                (q_any, q_ref),
                (gain_any, gain_ref),
                (scores_any, scores_ref),
                (wg_any.at[0], wg),
                (wu_any.at[0], wu),
                (wd_any.at[0], wd),
                (wmix_any, wmix),
            )
        )
    ]
    for load in loads:
        load.start()

    mark("a_greet")
    barrier = pltpu.get_barrier_semaphore()

    def greet(o, carry):
        pl.semaphore_signal(barrier, inc=1, device_id=((me + o) % n_ep, tp), device_id_type=MESH)
        return carry

    lax.fori_loop(1, n_ep, greet, 0)
    for j in range(1, n_y):
        pl.semaphore_signal(
            barrier, inc=1, device_id=(me, y_peer(j) * 2 + core), device_id_type=MESH
        )
    pl.semaphore_signal(barrier, inc=1, device_id=(me, mate), device_id_type=MESH)

    mark("b_route")
    loads[0].wait()
    expert_row = lax.broadcasted_iota(jnp.int32, (n_ep, tokens), 0)
    first = jnp.where(expert_row == routes_ref[0:1, :], 1.0, 0.0)
    second = jnp.where(expert_row == routes_ref[1:2, :], 1.0, 0.0)
    earlier = jnp.where(
        lax.broadcasted_iota(jnp.int32, (tokens, tokens), 0)
        < lax.broadcasted_iota(jnp.int32, (tokens, tokens), 1),
        1.0,
        0.0,
    ).astype(BF)
    before = jnp.dot((first + second).astype(BF), earlier, preferred_element_type=F32)
    place = before + expert_row.astype(F32) * slots_per
    slot_a = jnp.sum(first * place, axis=0, keepdims=True).astype(jnp.int32)
    slot_b = jnp.sum(second * place, axis=0, keepdims=True).astype(jnp.int32)
    slot_row = lax.broadcasted_iota(jnp.int32, (slots, tokens), 0)
    pick_a = jnp.where(slot_row == slot_a, 1.0, 0.0).astype(BF)
    pick_b = jnp.where(slot_row == slot_b, 1.0, 0.0).astype(BF)
    mark("c_pack")
    loads[1].wait()
    sent = jnp.dot(pick_a + pick_b, x_ref[...], preferred_element_type=F32).astype(BF)
    x_out[...] = sent.reshape(x_out.shape)
    x_buf[tp, me] = x_out[me]

    def disp(peer, source):
        return pltpu.make_async_remote_copy(
            x_out.at[peer], x_buf.at[tp, source], di_s.at[peer], di_r.at[source],
            device_id=(peer, tp), device_id_type=MESH,
        )

    def over_y(j, source, owner):
        return pltpu.make_async_remote_copy(
            x_buf.at[owner * 2 + core, source], x_buf.at[owner * 2 + core, source],
            dy_s.at[y_peer(j), source], dy_r.at[owner, source],
            device_id=(me, y_peer(j) * 2 + core), device_id_type=MESH,
        )

    def x_peer(i):
        return my_z * n_x + (my_x + i) % n_x

    def kv_send(peer, origin, sem):
        return pltpu.make_async_remote_copy(
            kv_buf.at[origin], kv_buf.at[origin], sem, kv_r.at[origin],
            device_id=(peer, tp), device_id_type=MESH,
        )

    def own_kv_right():
        return kv_send((my_z + 1) % n_z * n_x + my_x, me, kvz_s.at[my_z, 0])

    def own_kv_left():
        return kv_send((my_z + n_z - 1) % n_z * n_x + my_x, me, kvz_s.at[my_z, 1])

    mark("d_barrier")
    pl.semaphore_wait(barrier, n_ep - 1 + n_y)

    mark("e_disp")
    def dispatch(o):
        def start_disp(i, carry):
            disp(ep_other(o, i), me).start()
            return carry

        lax.fori_loop(1 if o == 0 else 0, n_x, start_disp, 0)

    at_end = jnp.logical_or(my_z == 0, my_z == n_z - 1)
    dispatch(0)
    dispatch(1)

    @pl.when(jnp.logical_not(at_end))
    def _():
        for o in range(2, n_z):
            dispatch(o)

    for j in range(1, n_y):
        over_y(j, me, my_y).start()

    mark("f_prepk")
    cos_table, sin_table = angle_tables(me * rows, rows)
    for i in (2, 3, 4):
        loads[i].wait()
    odd = kv_head % 2 == 1
    key = k_in[...].astype(F32)
    value = v_in[...].astype(F32)
    key = jnp.where(odd, pltpu.roll(key, HD, 1), key)
    value = jnp.where(odd, value, pltpu.roll(value, HD, 1))
    turned = prep(key, kg_ref[...], cos_table, sin_table)
    lane = lax.broadcasted_iota(jnp.int32, key.shape, 1)
    kv_buf[me] = jnp.where(lane < HD, turned, value).astype(BF)

    for i in range(1, n_x):
        kv_send(x_peer(i), me, kvx_s.at[my_z, i]).start()

    @pl.when(my_z < n_z - 1)
    def _():
        own_kv_right().start()

    @pl.when(my_z > 0)
    def _():
        own_kv_left().start()

    @pl.when(at_end)
    def _():
        for o in range(2, n_z):
            dispatch(o)

    side = my_z // (n_z // 2)
    outward = 1 - 2 * side
    inner = my_z + side * (n_z - 1 - 2 * my_z)

    def z_near(k):
        step = jnp.where(
            k <= 2 * inner, (k + 1) // 2 * (-1 if k % 2 else 1), k - inner
        )
        return my_z + outward * step

    def kv_pass(t, way):
        z = my_z - way * t
        there = jnp.logical_and(z >= 0, z < n_z)
        onward = my_z + way
        beyond = jnp.logical_and(onward >= 0, onward < n_z)
        z, onward = (z + n_z) % n_z, (onward + n_z) % n_z
        return there, beyond, z, kv_send(onward * n_x + my_x, z * n_x + my_x, kvz_s.at[z, 0])

    def kv_forward(t, way, ends):
        there, beyond, z, onward = kv_pass(t, way)
        origin = z * n_x + my_x

        @pl.when(jnp.logical_and(there, jnp.logical_not(beyond) if ends else beyond))
        def _():
            kv_send(origin, origin, kvz_s.at[z, 0]).wait_recv()
            if not ends:
                onward.start()
            for i in range(1, n_x):
                kv_send(x_peer(i), origin, kvx_s.at[z, i]).start()

    mark("f_prepq")
    factor = HD ** (-0.5) * math.log2(math.e)
    loads[5].wait()
    loads[6].wait()
    for tile in range(q_ref.shape[1] // LANES):
        q_tile = factor * prep(
            q_ref[:, tile * LANES:(tile + 1) * LANES].astype(F32),
            qg_ref[...], cos_table, sin_table,
        )
        q_lane = lax.broadcasted_iota(jnp.int32, q_tile.shape, 1)
        for part in range(2):
            head = tile * 2 + part
            if head < heads:
                moved = q_tile if part == 0 else pltpu.roll(q_tile, HD, 1)
                q_buf[head] = jnp.where(q_lane < HD, moved, 0.0).astype(BF)

    piece = rows // n_y
    half = piece // 2
    pieces = my_s.shape[1]

    def attend(block, count, start, many, fresh=False):
        at = pl.ds(pl.multiple_of(start, half), many)
        q_rows = q_buf[:, at, :].reshape(heads * many, LANES)
        kv = kv_buf[pl.ds(block, count)].reshape(count * rows, LANES)
        logits = lax.dot_general(
            q_rows, kv, (((1,), (1,)), ((), ())), preferred_element_type=F32
        )
        weights = jnp.exp2(logits).astype(BF)
        kv_lane = lax.broadcasted_iota(jnp.int32, kv.shape, 1)
        values = jnp.where(kv_lane < HD, jnp.ones_like(kv), kv)
        part = jnp.dot(weights, values, preferred_element_type=F32).reshape(heads, many, LANES)
        acc[:, at, :] = part if fresh else acc[:, at, :] + part

    def attend_all(block, fresh=False):
        def one(owner, carry):
            attend(block, 1, owner * piece, piece, fresh)
            return carry

        lax.fori_loop(0, n_y, one, 0)

    def kv_arrived(origin):
        kv_send(origin, origin, kvx_s.at[0, 0]).wait_recv()

    def others_attend(z):
        def one(i, carry):
            origin = z * n_x + (my_x + i) % n_x
            kv_arrived(origin)
            attend_all(origin)
            return carry

        lax.fori_loop(1, n_x, one, 0)

    def members(s):
        return pl.ds(z_other(s) * n_x, n_x)

    def group_rows(o):
        return pl.ds(pl.multiple_of(z_other(o) * group, group), group)

    def to_mate(owner, mine, s):
        part = x_buf.at[owner * 2 + mine, members(s)]
        return pltpu.make_async_remote_copy(
            part, part, dc_s.at[owner, s], dc_r.at[owner, s],
            device_id=(me, mate), device_id_type=MESH,
        )

    def pass_on(o):
        def one(i, carry):
            source = ep_other(o, i)
            disp(source, source).wait_recv()
            for j in range(1, n_y):
                over_y(j, source, my_y).start()
            return carry

        lax.fori_loop(1 if o == 0 else 0, n_x, one, 0)
        to_mate(my_y, core, o).start()

    def from_y(s):
        for j in range(1, n_y):
            owner = y_peer(j)

            def arrived(i, carry):
                over_y(j, z_other(s) * n_x + i, owner).wait_recv()
                return carry

            lax.fori_loop(0, n_x, arrived, 0)
            to_mate(owner, core, s).start()

    def expert_in(s):
        for j in range(n_y):
            to_mate(y_peer(j), 1 - core, s).wait_recv()
        count = group
        power = jnp.zeros((count, 1), F32)
        for q in range(n_tp):
            x_q = x_buf[q, members(s)].reshape(count, col_w).astype(F32)
            power = power + jnp.sum(x_q * x_q, axis=1, keepdims=True)
            scaled[group_rows(s), q * col_w:(q + 1) * col_w] = (
                x_q * gain_ref[:, q * col_w:(q + 1) * col_w]
            ).astype(BF)
        return lax.rsqrt(power * (1.0 / model_width) + EPSILON)

    hidden_w = wg.shape[1]
    tile_w = math.gcd(hidden_w, 1024)

    def expert_hidden(s, row_scale):
        at = group_rows(s)

        def hidden_tile(i, carry):
            cols = pl.ds(pl.multiple_of(i * tile_w, tile_w), tile_w)
            gate = row_scale * jnp.dot(scaled[at, :], wg[:, cols], preferred_element_type=F32)
            up = row_scale * jnp.dot(scaled[at, :], wu[:, cols], preferred_element_type=F32)
            hid[at, cols] = (gate / (1.0 + jnp.exp(-gate)) * up).astype(BF)
            return carry

        lax.fori_loop(0, hidden_w // tile_w, hidden_tile, 0)

    def expert_mate(owner, side, o):
        return pltpu.make_async_remote_copy(
            dp_buf.at[owner * 2 + side, group_rows(o)], ep_in.at[owner, group_rows(o)],
            ep_s.at[owner, o], ep_r.at[owner, o],
            device_id=(me, mate), device_id_type=MESH,
        )

    def expert_y(j, origin, o):
        return pltpu.make_async_remote_copy(
            es_buf.at[y_peer(j), group_rows(o)], ey_in.at[origin, group_rows(o)],
            ey_s.at[y_peer(j), o], ey_r.at[origin, o],
            device_id=(me, y_peer(j) * 2 + core), device_id_type=MESH,
        )

    def expert_down(s):
        at = group_rows(s)
        total = jnp.dot(hid[at, :], wd[...], preferred_element_type=F32).astype(BF)
        for q in range(n_tp):
            dp_buf[q, at] = total[:, q * col_w:(q + 1) * col_w]
        for j in range(1, n_y + 1):
            expert_mate(y_peer(j), 1 - core, s).start()

    def mate_sum(j, o):
        owner = y_peer(j)
        expert_mate(owner, core, o).wait_recv()
        at = group_rows(o)
        return dp_buf[owner * 2 + core, at].astype(F32) + ep_in[owner, at].astype(F32)

    def expert_send(s):
        for j in range(1, n_y):
            es_buf[y_peer(j), group_rows(s)] = mate_sum(j, s).astype(BF)
            expert_y(j, my_y, s).start()

    def ret(peer, origin):
        return pltpu.make_async_remote_copy(
            ret_out.at[peer], ret_in.at[origin], rt_s.at[peer], rt_r.at[origin],
            device_id=(peer, tp), device_id_type=MESH,
        )

    def expert_return(o):
        total = mate_sum(0, o)
        for j in range(1, n_y):
            expert_y(j, y_peer(j), o).wait_recv()
            total = total + ey_in[y_peer(j), group_rows(o)].astype(F32)
        ret_out[pl.ds(z_other(o) * n_x, n_x)] = total.astype(BF).reshape(n_x, slots_per, col_w)

        def one(i, carry):
            ret(ep_other(o, i), me).start()
            return carry

        lax.fori_loop(0 if o else 1, n_x, one, 0)
        if o == 0:
            ret_in[me] = ret_out[me]

    def mix_mate(owner, side):
        return pltpu.make_async_remote_copy(
            mp_out.at[owner, side], mp_in.at[owner], mp_s.at[owner], mp_r.at[owner],
            device_id=(me, mate), device_id_type=MESH,
        )

    def mix_y(j, origin, c):
        at = pl.ds(c * (half // pieces), half // pieces)
        return pltpu.make_async_remote_copy(
            ms_out.at[y_peer(j), at], my_in.at[origin, at], my_s.at[y_peer(j), c], my_r.at[origin, c],
            device_id=(me, y_peer(j) * 2 + core), device_id_type=MESH,
        )

    def mix(owner, whose):
        start = pl.multiple_of(owner * piece + whose * half, half)
        total = acc[:, pl.ds(start, half), :].reshape(heads * half, LANES)
        ratio = (total / pltpu.roll(total, HD, 1)).reshape(heads, half, LANES)
        out_lane = lax.broadcasted_iota(jnp.int32, (half, LANES), 1)
        tiles = []
        for tile in range(q_ref.shape[1] // LANES):
            left = pltpu.roll(ratio[2 * tile], HD, 1)
            right = ratio[2 * tile + 1] if 2 * tile + 1 < heads else jnp.zeros_like(left)
            tiles.append(jnp.where(out_lane < HD, left, right).astype(BF))
        attended = tiles[0] if len(tiles) == 1 else jnp.concatenate(tiles, axis=1)
        mp_out[owner, whose] = jnp.dot(attended, wmix[...], preferred_element_type=F32).astype(BF)

    def mix_sum(owner):
        mix_mate(owner, core).wait_recv()
        return mp_out[owner, core].astype(F32) + mp_in[owner].astype(F32)

    def near_arrived(k):
        for i in range(1, n_x):
            kv_arrived(z_near(k) * n_x + (my_x + i) % n_x)

    others = [y_peer(j) for j in range(1, n_y)]

    def attend_first(k, owners):
        for owner in owners:
            attend(z_near(k) * n_x + my_x, 1, owner * piece, piece)

    def attend_second(k, owners):
        def one(i, carry):
            for owner in owners:
                attend(z_near(k) * n_x + (my_x + i) % n_x, 1, owner * piece, piece)
            return carry

        lax.fori_loop(1, n_x, one, 0)

    def attend_both(k, start, many):
        attend(z_near(k) * n_x, n_x, start, many)

    def expert_rows(s):
        mark(f"in{s}")
        row_scale = expert_in(s)
        mark(f"hid{s}")
        expert_hidden(s, row_scale)

    mark("g_attown")
    attend_all(me, True)
    mark("g_pass0")
    pass_on(0)
    mark("g_pass1")
    pass_on(1)
    mark("fromy0")
    from_y(0)
    mark("kva")
    kv_forward(1, outward, False)
    kv_forward(1, -outward, True)
    mark("attownx")
    others_attend(my_z)
    loads[7].wait()
    loads[9].wait()
    loads[10].wait()
    loads[11].wait()
    expert_rows(0)
    mark("fromy1")
    from_y(1)
    mark("pass2")
    pass_on(2)
    mark("down0")
    expert_down(0)
    mark("in1")
    row_scale = expert_in(1)
    mark("kvf1")
    kv_forward(1, -outward, False)
    mark("hid1")
    expert_hidden(1, row_scale)
    mark("pass3")
    pass_on(3)
    mark("down1")
    expert_down(1)
    mark("att1")
    attend_first(1, others)
    mark("send0")
    expert_send(0)
    for s in range(2, n_z):
        if s > 2:
            mark(f"pass{s+1}")
            if s + 1 < n_z:
                pass_on(s + 1)
        mark(f"send{s-1}")
        expert_send(s - 1)
        mark(f"fromy{s}")
        from_y(s)
        mark(f"kvf{s}")
        if s < n_z // 2:
            kv_forward(s, outward, False)
        if s < n_z - 1:
            kv_forward(s, -outward, False)
        if s == 2:
            mark("att1x")
            near_arrived(1)
            attend_second(1, others)
        if s == 3:
            mark("att2")
            attend_first(2, others)
        if s == n_z - 1:
            mark(f"kvg{s}")
            kv_forward(s, -outward, True)
        mark(f"in{s}")
        row_scale = expert_in(s)
        mark(f"hid{s}")
        expert_hidden(s, row_scale)
        mark(f"down{s}")
        expert_down(s)
        if s < n_z - 1:
            mark(f"kvg{s}")
            kv_forward(s, -outward, True)
    mark("att2x")
    near_arrived(2)
    attend_second(2, others)
    mark("send")
    expert_send(n_z - 1)
    mark("ret0")
    expert_return(0)
    expert_return(1)
    loads[12].wait()
    mark("arr3")
    for k in range(3, n_z):
        near_arrived(k)
    for whose in (1 - core, core):
        if whose is core:
            mark("ret2")
            for o in range(2, n_z - 1):
                expert_return(o)
        for owner in others:
            mark("att3")
            for k in range(3, n_z):
                attend_both(k, owner * piece + whose * half, half)
            mark("mix")
            mix(owner, whose)
            if whose is not core:
                mix_mate(owner, 1 - core).start()
    mark("k_mixsum")
    for j in range(1, n_y):
        ms_out[y_peer(j)] = mix_sum(y_peer(j)).astype(BF)
        for c in range(pieces):
            mix_y(j, my_y, c).start()
    mark("k_ret")
    expert_return(n_z - 1)
    mark("k_att2")

    for k in range(1, n_z):
        attend_both(k, my_y * piece, piece)
    mark("k_mix")
    mix(my_y, 1 - core)
    mix_mate(my_y, 1 - core).start()
    mix(my_y, core)

    mark("l_retwait")

    def ret_wait(o, carry):
        source = (me + n_ep - o) % n_ep
        ret(source, source).wait_recv()
        return carry

    lax.fori_loop(1, n_ep, ret_wait, 0)
    mark("m_combine")
    loads[8].wait()
    back = ret_in[...].reshape(slots, col_w)
    share_row = scores_ref[...] / jnp.sum(scores_ref[...], axis=0, keepdims=True)
    own_token = lax.broadcasted_iota(jnp.int32, (tokens, tokens), 0) == lax.broadcasted_iota(
        jnp.int32, (tokens, tokens), 1
    )
    share_a, share_b = (
        jnp.sum(jnp.where(own_token, share_row[i:i + 1, :], 0.0), axis=1, keepdims=True)
        for i in range(2)
    )
    rows_a = lax.dot_general(
        pick_a, back, (((0,), (0,)), ((), ())), preferred_element_type=F32
    )
    rows_b = lax.dot_general(
        pick_b, back, (((0,), (0,)), ((), ())), preferred_element_type=F32
    )
    out_ref[...] = (rows_a * share_a + rows_b * share_b).astype(BF)

    mark("n_mixsum")
    total = mix_sum(my_y)
    mark("n_ywait")
    for j in range(1, n_y):
        for c in range(pieces):
            mix_y(j, y_peer(j), c).wait_recv()
        total = total + my_in[y_peer(j)].astype(F32)
    mark("n_out")
    mixed_ref[...] = total.astype(BF)

    mark("o_sends")

    def sends(o, carry):
        peer = (me + o) % n_ep
        disp(peer, me).wait_send()
        ret(peer, me).wait_send()
        return carry

    lax.fori_loop(1, n_ep, sends, 0)
    for i in range(1, n_x):

        def sent_x(z, carry):
            kv_send(x_peer(i), z * n_x + my_x, kvx_s.at[z, i]).wait_send()
            return carry

        lax.fori_loop(0, n_z, sent_x, 0)

    @pl.when(my_z < n_z - 1)
    def _():
        own_kv_right().wait_send()

    @pl.when(my_z > 0)
    def _():
        own_kv_left().wait_send()

    for t in range(1, n_z):
        for way in (outward, -outward):
            there, beyond, z, onward = kv_pass(t, way)

            @pl.when(jnp.logical_and(there, beyond))
            def _():
                onward.wait_send()

    for j in range(1, n_y):

        def sent_y(source, carry):
            over_y(j, source, my_y).wait_send()
            return carry

        lax.fori_loop(0, n_ep, sent_y, 0)
        for c in range(pieces):
            mix_y(j, my_y, c).wait_send()
    for j in range(n_y):
        for s in range(stages):
            to_mate(y_peer(j), core, s).wait_send()
        for o in range(n_z):
            expert_mate(y_peer(j), 1 - core, o).wait_send()
            if j:
                expert_y(j, my_y, o).wait_send()
        mix_mate(y_peer(j), 1 - core).wait_send()
    mark(None)


def local(
    n_ep, n_tp,
    queries, key_input, value_input, query_gain, key_gain, mix_out_weight, expert_input, ffn_gain,
    routes, route_scores, gate_weight, up_weight, down_weight,
):
    rows = queries.shape[0]
    heads = queries.shape[1] // HD
    n_y = n_tp // 2
    n_x = 1 << ((n_ep.bit_length() - 1) // 2)
    n_z = n_ep // n_x
    stages = n_z
    spare = heads % 2 * HD
    if spare:
        queries = jnp.pad(queries, ((0, 0), (0, spare)))
        mix_out_weight = jnp.pad(mix_out_weight, ((0, spare), (0, 0)))
    width = expert_input.shape[1]
    col_w = width // n_tp
    tokens, top = routes.shape
    capacity = 3 * tokens * top // (2 * n_ep)
    slots_per = -(-capacity // 16) * 16
    slots = n_ep * slots_per
    hidden_w = gate_weight.shape[2]
    out_w = mix_out_weight.shape[1]
    half = rows // n_tp
    vm = pltpu.VMEM
    dma = pltpu.SemaphoreType.DMA
    scratch = [
        vm(queries.shape, BF), vm((rows, LANES), BF), vm((rows, LANES), BF), vm((tokens, col_w), BF),
        vm((1, HD), F32), vm((1, HD), F32), vm((1, width), F32), vm((top, tokens), jnp.int32), vm((top, tokens), F32),
        vm((width, hidden_w), BF), vm((width, hidden_w), BF), vm((hidden_w, width), BF),
        vm(mix_out_weight.shape, BF),
        vm((n_ep, rows, LANES), BF), vm((heads, rows, LANES), BF), vm((heads, rows, LANES), F32),
        vm((n_ep, slots_per, col_w), BF), vm((n_tp, n_ep, slots_per, col_w), BF),
        vm((slots, width), BF), vm((slots, hidden_w), BF),
        vm((n_tp, slots, col_w), BF), vm((n_y, slots, col_w), BF), vm((n_y, slots, col_w), BF),
        vm((n_y, slots, col_w), BF),
        vm((n_ep, slots_per, col_w), BF), vm((n_ep, slots_per, col_w), BF),
        vm((n_y, 2, half, out_w), BF), vm((n_y, half, out_w), BF), vm((n_y, half, out_w), BF),
        vm((n_y, half, out_w), BF),
        dma((13,)),
        dma((n_z, n_x)), dma((n_z, 2)), dma((n_ep,)), dma((n_ep,)), dma((n_ep,)),
        dma((n_y, n_ep)), dma((n_y, n_ep)),
    ] + [dma((n_y, stages))] * 2 + [dma((n_y, n_z))] * 4 + [dma((n_ep,))] * 2 + [dma((n_y,))] * 2 + [dma((n_y, 2))] * 2
    in_vmem = pl.BlockSpec(memory_space=pltpu.VMEM)
    in_hbm = pl.BlockSpec(memory_space=pltpu.HBM)
    return pl.pallas_call(
        functools.partial(kernel, n_ep, n_tp, heads, width),
        out_shape=(
            pltpu.VMEM((half, out_w), BF),
            pltpu.VMEM((tokens, col_w), BF),
        ),
        in_specs=[in_hbm] * 13,
        out_specs=(in_vmem, in_vmem),
        scratch_shapes=scratch,
        compiler_params=pltpu.CompilerParams(
            collective_id=0, has_side_effects=True, vmem_limit_bytes=56 * 1024 * 1024
        ),
    )(
        queries, key_input, value_input, query_gain[None, :], key_gain[None, :],
        mix_out_weight, expert_input, ffn_gain[None, :], routes.T, route_scores.T,
        gate_weight, up_weight, down_weight,
    )


def solution(mesh):
    placed = (
        P("ep", "tp"),
        P("ep", None),
        P("ep", None),
        P(),
        P(),
        P("tp", None),
        P("ep", None),
        P(),
        P("ep", None),
        P("ep", None),
        P("ep", None, "tp"),
        P("ep", None, "tp"),
        P("ep", "tp", None),
    )
    return jax.shard_map(
        functools.partial(local, mesh.shape["ep"], mesh.shape["tp"]),
        mesh=mesh,
        in_specs=placed,
        out_specs=(P(("ep", "tp"), None), P("ep", "tp")),
        check_vma=False,
    )
```

```python
import functools
import math

import jax
import jax.numpy as jnp
from jax import lax
from jax.experimental import pallas as pl
from jax.experimental.pallas import tpu as pltpu
from jax.sharding import PartitionSpec as P

HEADS = 16
KV_HEADS = 4
HD = 64
GRID_W = 64
EPSILON = 1e-06
ROPE_BASE = 10000.0
MESH = pl.DeviceIdType.MESH
LANES = 128
BF = jnp.bfloat16
F32 = jnp.float32


def prep(values, gain, cos_table, sin_table):
    width = values.shape[1]
    squares = values * values
    high = squares.astype(BF)
    low = (squares - high.astype(F32)).astype(BF)
    rows = lax.broadcasted_iota(jnp.int32, (width, width), 0) // HD
    cols = lax.broadcasted_iota(jnp.int32, (width, width), 1) // HD
    same = jnp.where(rows == cols, 1.0, 0.0).astype(BF)
    total = jnp.dot(high, same, preferred_element_type=F32) + jnp.dot(
        low, same, preferred_element_type=F32
    )
    gain = jnp.concatenate([gain] * (width // HD), axis=1)
    normed = values * lax.rsqrt(total * (1.0 / HD) + EPSILON) * gain
    lane = lax.broadcasted_iota(jnp.int32, normed.shape, 1)
    quarter = HD // 4
    partner = jnp.where(
        lane % (2 * quarter) < quarter,
        pltpu.roll(normed, width - quarter, 1),
        pltpu.roll(normed, quarter, 1),
    )
    return normed * cos_table + partner * sin_table


def angle_tables(start, rows):
    quarter = HD // 4
    many = rows // GRID_W

    def both(count, first):
        shape = (count, LANES)
        place = lax.broadcasted_iota(jnp.int32, shape, 0) + first
        lane = lax.broadcasted_iota(jnp.int32, shape, 1)
        turn = lane % quarter
        inverse = jnp.zeros(shape, F32)
        for j in range(quarter):
            inverse = jnp.where(turn == j, ROPE_BASE ** (-j / quarter), inverse)
        angle = place.astype(F32) * inverse
        sign = jnp.where(lane % (2 * quarter) < quarter, -1.0, 1.0)
        return jnp.cos(angle), jnp.sin(angle) * sign

    tables = []
    for by_row, by_col in zip(both(max(many, 8), start // GRID_W), both(GRID_W, 0)):
        lane = lax.broadcasted_iota(jnp.int32, by_col.shape, 1)
        tables.append(
            jnp.concatenate(
                [jnp.where(lane % HD < HD // 2, by_row[i:i + 1, :], by_col) for i in range(many)],
                axis=0,
            )
        )
    return tables


def mark(name):
    pass


def kernel(
    n_ep, n_tp, heads, model_width,
    q_any, k_any, v_any, qg_any, kg_any, wmix_any, x_any, gain_any, routes_any, scores_any, wg_any, wu_any, wd_any,
    mixed_ref, out_ref,
    q_ref, k_in, v_in, x_ref, qg_ref, kg_ref, gain_ref, routes_ref, scores_ref, wg, wu, wd, wmix,
    kv_buf, q_buf, acc, x_out, x_buf, scaled, hid, dp_buf, ep_in, es_buf, ey_in,
    ret_out, ret_in, mp_out, mp_in, ms_out, my_in,
    w_sem, kvx_s, kvz_s, kv_r, di_s, di_r, dy_s, dy_r, dc_s, dc_r, ep_s, ep_r, ey_s, ey_r, rt_s, rt_r,
    mp_s, mp_r, my_s, my_r,
):
    n_y = n_tp // 2
    n_x = 1 << ((n_ep.bit_length() - 1) // 2)
    n_z = n_ep // n_x
    stages = n_z
    me = lax.axis_index("ep")
    tp = lax.axis_index("tp")
    my_y, core = tp // 2, tp % 2
    my_z, my_x = me // n_x, me % n_x
    mate = my_y * 2 + 1 - core
    rows = q_ref.shape[0]
    kv_head = tp * heads // (HEADS // KV_HEADS)
    kv_tile = pl.ds(pl.multiple_of(kv_head // 2 * LANES, LANES), LANES)
    slots_per, col_w = x_buf.shape[2:]
    slots = n_ep * slots_per
    group = n_x * slots_per
    tokens = x_ref.shape[0]
    x_cols = pl.ds(pl.multiple_of(tp * col_w, col_w), col_w)

    def y_peer(j):
        return (my_y + j) % n_y

    def z_other(o):
        z = my_z
        for bit in range(n_z.bit_length() - 1):
            if o >> bit & 1:
                z = z + (1 - 2 * (my_z // (1 << bit) % 2)) * (1 << bit)
        return z

    def ep_other(o, i):
        return z_other(o) * n_x + (my_x + i) % n_x

    loads = [
        pltpu.make_async_copy(src, dst, w_sem.at[i])
        for i, (src, dst) in enumerate(
            (
                (routes_any, routes_ref),
                (x_any.at[:, x_cols], x_ref),
                (kg_any, kg_ref),
                (k_any.at[:, kv_tile], k_in),
                (v_any.at[:, kv_tile], v_in),
                (qg_any, qg_ref),
                (q_any, q_ref),
                (gain_any, gain_ref),
                (scores_any, scores_ref),
                (wg_any.at[0], wg),
                (wu_any.at[0], wu),
                (wd_any.at[0], wd),
                (wmix_any, wmix),
            )
        )
    ]
    for load in loads:
        load.start()

    mark("a_greet")
    barrier = pltpu.get_barrier_semaphore()

    def greet(o, carry):
        pl.semaphore_signal(barrier, inc=1, device_id=((me + o) % n_ep, tp), device_id_type=MESH)
        return carry

    lax.fori_loop(1, n_ep, greet, 0)
    for j in range(1, n_y):
        pl.semaphore_signal(
            barrier, inc=1, device_id=(me, y_peer(j) * 2 + core), device_id_type=MESH
        )
    pl.semaphore_signal(barrier, inc=1, device_id=(me, mate), device_id_type=MESH)

    mark("b_route")
    cos_table, sin_table = angle_tables(me * rows, rows)
    loads[0].wait()
    expert_row = lax.broadcasted_iota(jnp.int32, (n_ep, tokens), 0)
    first = jnp.where(expert_row == routes_ref[0:1, :], 1.0, 0.0)
    second = jnp.where(expert_row == routes_ref[1:2, :], 1.0, 0.0)
    earlier = jnp.where(
        lax.broadcasted_iota(jnp.int32, (tokens, tokens), 0)
        < lax.broadcasted_iota(jnp.int32, (tokens, tokens), 1),
        1.0,
        0.0,
    ).astype(BF)
    before = jnp.dot((first + second).astype(BF), earlier, preferred_element_type=F32)
    place = before + expert_row.astype(F32) * slots_per
    slot_a = jnp.sum(first * place, axis=0, keepdims=True).astype(jnp.int32)
    slot_b = jnp.sum(second * place, axis=0, keepdims=True).astype(jnp.int32)
    slot_row = lax.broadcasted_iota(jnp.int32, (slots, tokens), 0)
    pick_a = jnp.where(slot_row == slot_a, 1.0, 0.0).astype(BF)
    pick_b = jnp.where(slot_row == slot_b, 1.0, 0.0).astype(BF)
    mark("c_pack")
    loads[1].wait()
    sent = jnp.dot(pick_a + pick_b, x_ref[...], preferred_element_type=F32).astype(BF)
    x_out[...] = sent.reshape(x_out.shape)
    x_buf[tp, me] = x_out[me]

    def disp(peer, source):
        return pltpu.make_async_remote_copy(
            x_out.at[peer], x_buf.at[tp, source], di_s.at[peer], di_r.at[source],
            device_id=(peer, tp), device_id_type=MESH,
        )

    def over_y(j, source, owner):
        return pltpu.make_async_remote_copy(
            x_buf.at[owner * 2 + core, source], x_buf.at[owner * 2 + core, source],
            dy_s.at[y_peer(j), source], dy_r.at[owner, source],
            device_id=(me, y_peer(j) * 2 + core), device_id_type=MESH,
        )

    def x_peer(i):
        return my_z * n_x + (my_x + i) % n_x

    def kv_send(peer, origin, sem):
        return pltpu.make_async_remote_copy(
            kv_buf.at[origin], kv_buf.at[origin], sem, kv_r.at[origin],
            device_id=(peer, tp), device_id_type=MESH,
        )

    def own_kv_right():
        return kv_send((my_z + 1) % n_z * n_x + my_x, me, kvz_s.at[my_z, 0])

    def own_kv_left():
        return kv_send((my_z + n_z - 1) % n_z * n_x + my_x, me, kvz_s.at[my_z, 1])

    mark("d_barrier")
    pl.semaphore_wait(barrier, n_ep - 1 + n_y)

    mark("e_disp")
    def dispatch(o):
        def start_disp(i, carry):
            disp(ep_other(o, i), me).start()
            return carry

        lax.fori_loop(1 if o == 0 else 0, n_x, start_disp, 0)

    at_end = jnp.logical_or(my_z == 0, my_z == n_z - 1)
    dispatch(0)
    dispatch(1)

    @pl.when(jnp.logical_not(at_end))
    def _():
        dispatch(2)

    for j in range(1, n_y):
        over_y(j, me, my_y).start()

    mark("f_prepk")
    for i in (2, 3, 4):
        loads[i].wait()
    odd = kv_head % 2 == 1
    key = k_in[...].astype(F32)
    value = v_in[...].astype(F32)
    key = jnp.where(odd, pltpu.roll(key, HD, 1), key)
    value = jnp.where(odd, value, pltpu.roll(value, HD, 1))
    turned = prep(key, kg_ref[...], cos_table, sin_table)
    lane = lax.broadcasted_iota(jnp.int32, key.shape, 1)
    kv_buf[me] = jnp.where(lane < HD, turned, value).astype(BF)

    for i in range(1, n_x):
        kv_send(x_peer(i), me, kvx_s.at[my_z, i]).start()

    @pl.when(my_z < n_z - 1)
    def _():
        own_kv_right().start()

    @pl.when(my_z > 0)
    def _():
        own_kv_left().start()

    @pl.when(at_end)
    def _():
        dispatch(2)

    for o in range(3, n_z):
        dispatch(o)

    side = my_z // (n_z // 2)
    outward = 1 - 2 * side
    inner = my_z + side * (n_z - 1 - 2 * my_z)

    def z_near(k):
        step = jnp.where(
            k <= 2 * inner, (k + 1) // 2 * (-1 if k % 2 else 1), k - inner
        )
        return my_z + outward * step

    def kv_pass(t, way):
        z = my_z - way * t
        there = jnp.logical_and(z >= 0, z < n_z)
        onward = my_z + way
        beyond = jnp.logical_and(onward >= 0, onward < n_z)
        z, onward = (z + n_z) % n_z, (onward + n_z) % n_z
        return there, beyond, z, kv_send(onward * n_x + my_x, z * n_x + my_x, kvz_s.at[z, 0])

    def kv_forward(t, way, ends):
        there, beyond, z, onward = kv_pass(t, way)
        origin = z * n_x + my_x

        @pl.when(jnp.logical_and(there, jnp.logical_not(beyond) if ends else beyond))
        def _():
            kv_send(origin, origin, kvz_s.at[z, 0]).wait_recv()
            if not ends:
                onward.start()
            for i in range(1, n_x):
                kv_send(x_peer(i), origin, kvx_s.at[z, i]).start()

    mark("f_prepq")
    factor = HD ** (-0.5) * math.log2(math.e)
    loads[5].wait()
    loads[6].wait()
    for tile in range(q_ref.shape[1] // LANES):
        q_tile = factor * prep(
            q_ref[:, tile * LANES:(tile + 1) * LANES].astype(F32),
            qg_ref[...], cos_table, sin_table,
        )
        q_lane = lax.broadcasted_iota(jnp.int32, q_tile.shape, 1)
        for part in range(2):
            head = tile * 2 + part
            if head < heads:
                moved = q_tile if part == 0 else pltpu.roll(q_tile, HD, 1)
                q_buf[head] = jnp.where(q_lane < HD, moved, 0.0).astype(BF)

    piece = rows // n_y
    half = piece // 2
    pieces = my_s.shape[1]

    def attend(block, count, start, many, fresh=False):
        at = pl.ds(pl.multiple_of(start, half), many)
        q_rows = q_buf[:, at, :].reshape(heads * many, LANES)
        kv = kv_buf[pl.ds(block, count)].reshape(count * rows, LANES)
        logits = lax.dot_general(
            q_rows, kv, (((1,), (1,)), ((), ())), preferred_element_type=F32
        )
        weights = jnp.exp2(logits).astype(BF)
        kv_lane = lax.broadcasted_iota(jnp.int32, kv.shape, 1)
        values = jnp.where(kv_lane < HD, jnp.ones_like(kv), kv)
        part = jnp.dot(weights, values, preferred_element_type=F32).reshape(heads, many, LANES)
        acc[:, at, :] = part if fresh else acc[:, at, :] + part

    def attend_all(block, fresh=False):
        def one(owner, carry):
            attend(block, 1, owner * piece, piece, fresh)
            return carry

        lax.fori_loop(0, n_y, one, 0)

    def kv_arrived(origin):
        kv_send(origin, origin, kvx_s.at[0, 0]).wait_recv()

    def others_attend(z):
        def one(i, carry):
            origin = z * n_x + (my_x + i) % n_x
            kv_arrived(origin)
            attend_all(origin)
            return carry

        lax.fori_loop(1, n_x, one, 0)

    def members(s):
        return pl.ds(z_other(s) * n_x, n_x)

    def group_rows(o):
        return pl.ds(pl.multiple_of(z_other(o) * group, group), group)

    def to_mate(owner, mine, s):
        part = x_buf.at[owner * 2 + mine, members(s)]
        return pltpu.make_async_remote_copy(
            part, part, dc_s.at[owner, s], dc_r.at[owner, s],
            device_id=(me, mate), device_id_type=MESH,
        )

    def pass_on(o):
        def one(i, carry):
            source = ep_other(o, i)
            disp(source, source).wait_recv()
            for j in range(1, n_y):
                over_y(j, source, my_y).start()
            return carry

        lax.fori_loop(1 if o == 0 else 0, n_x, one, 0)
        to_mate(my_y, core, o).start()

    def from_y(s):
        for j in range(1, n_y):
            owner = y_peer(j)

            def arrived(i, carry):
                over_y(j, z_other(s) * n_x + i, owner).wait_recv()
                return carry

            lax.fori_loop(0, n_x, arrived, 0)
            to_mate(owner, core, s).start()

    def expert_in(s):
        for j in range(n_y):
            to_mate(y_peer(j), 1 - core, s).wait_recv()
        count = group
        power = jnp.zeros((count, 1), F32)
        for q in range(n_tp):
            x_q = x_buf[q, members(s)].reshape(count, col_w).astype(F32)
            power = power + jnp.sum(x_q * x_q, axis=1, keepdims=True)
            scaled[group_rows(s), q * col_w:(q + 1) * col_w] = (
                x_q * gain_ref[:, q * col_w:(q + 1) * col_w]
            ).astype(BF)
        return lax.rsqrt(power * (1.0 / model_width) + EPSILON)

    hidden_w = wg.shape[1]
    tile_w = math.gcd(hidden_w, 1024)

    def expert_hidden(s, row_scale):
        at = group_rows(s)

        def hidden_tile(i, carry):
            cols = pl.ds(pl.multiple_of(i * tile_w, tile_w), tile_w)
            gate = row_scale * jnp.dot(scaled[at, :], wg[:, cols], preferred_element_type=F32)
            up = row_scale * jnp.dot(scaled[at, :], wu[:, cols], preferred_element_type=F32)
            hid[at, cols] = (gate / (1.0 + jnp.exp(-gate)) * up).astype(BF)
            return carry

        lax.fori_loop(0, hidden_w // tile_w, hidden_tile, 0)

    def expert_mate(owner, side, o):
        return pltpu.make_async_remote_copy(
            dp_buf.at[owner * 2 + side, group_rows(o)], ep_in.at[owner, group_rows(o)],
            ep_s.at[owner, o], ep_r.at[owner, o],
            device_id=(me, mate), device_id_type=MESH,
        )

    def expert_y(j, origin, o):
        return pltpu.make_async_remote_copy(
            es_buf.at[y_peer(j), group_rows(o)], ey_in.at[origin, group_rows(o)],
            ey_s.at[y_peer(j), o], ey_r.at[origin, o],
            device_id=(me, y_peer(j) * 2 + core), device_id_type=MESH,
        )

    def expert_down(s):
        at = group_rows(s)
        total = jnp.dot(hid[at, :], wd[...], preferred_element_type=F32).astype(BF)
        for q in range(n_tp):
            dp_buf[q, at] = total[:, q * col_w:(q + 1) * col_w]
        for j in range(1, n_y + 1):
            expert_mate(y_peer(j), 1 - core, s).start()

    def mate_sum(j, o):
        owner = y_peer(j)
        expert_mate(owner, core, o).wait_recv()
        at = group_rows(o)
        return dp_buf[owner * 2 + core, at].astype(F32) + ep_in[owner, at].astype(F32)

    def expert_send(s):
        for j in range(1, n_y):
            es_buf[y_peer(j), group_rows(s)] = mate_sum(j, s).astype(BF)
            expert_y(j, my_y, s).start()

    def ret(peer, origin):
        return pltpu.make_async_remote_copy(
            ret_out.at[peer], ret_in.at[origin], rt_s.at[peer], rt_r.at[origin],
            device_id=(peer, tp), device_id_type=MESH,
        )

    def expert_return(o):
        total = mate_sum(0, o)
        for j in range(1, n_y):
            expert_y(j, y_peer(j), o).wait_recv()
            total = total + ey_in[y_peer(j), group_rows(o)].astype(F32)
        ret_out[pl.ds(z_other(o) * n_x, n_x)] = total.astype(BF).reshape(n_x, slots_per, col_w)

        def one(i, carry):
            ret(ep_other(o, i), me).start()
            return carry

        lax.fori_loop(0 if o else 1, n_x, one, 0)
        if o == 0:
            ret_in[me] = ret_out[me]

    def mix_mate(owner, side):
        return pltpu.make_async_remote_copy(
            mp_out.at[owner, side], mp_in.at[owner], mp_s.at[owner], mp_r.at[owner],
            device_id=(me, mate), device_id_type=MESH,
        )

    def mix_y(j, origin, c):
        at = pl.ds(c * (half // pieces), half // pieces)
        return pltpu.make_async_remote_copy(
            ms_out.at[y_peer(j), at], my_in.at[origin, at], my_s.at[y_peer(j), c], my_r.at[origin, c],
            device_id=(me, y_peer(j) * 2 + core), device_id_type=MESH,
        )

    def mix(owner, whose):
        start = pl.multiple_of(owner * piece + whose * half, half)
        total = acc[:, pl.ds(start, half), :].reshape(heads * half, LANES)
        ratio = (total / pltpu.roll(total, HD, 1)).reshape(heads, half, LANES)
        out_lane = lax.broadcasted_iota(jnp.int32, (half, LANES), 1)
        tiles = []
        for tile in range(q_ref.shape[1] // LANES):
            left = pltpu.roll(ratio[2 * tile], HD, 1)
            right = ratio[2 * tile + 1] if 2 * tile + 1 < heads else jnp.zeros_like(left)
            tiles.append(jnp.where(out_lane < HD, left, right).astype(BF))
        attended = tiles[0] if len(tiles) == 1 else jnp.concatenate(tiles, axis=1)
        mp_out[owner, whose] = jnp.dot(attended, wmix[...], preferred_element_type=F32).astype(BF)

    def mix_sum(owner):
        mix_mate(owner, core).wait_recv()
        return mp_out[owner, core].astype(F32) + mp_in[owner].astype(F32)

    def near_arrived(k):
        for i in range(1, n_x):
            kv_arrived(z_near(k) * n_x + (my_x + i) % n_x)

    others = [y_peer(j) for j in range(1, n_y)]

    def attend_first(k, owners):
        for owner in owners:
            attend(z_near(k) * n_x + my_x, 1, owner * piece, piece)

    def attend_second(k, owners):
        def one(i, carry):
            for owner in owners:
                attend(z_near(k) * n_x + (my_x + i) % n_x, 1, owner * piece, piece)
            return carry

        lax.fori_loop(1, n_x, one, 0)

    def attend_both(k, start, many):
        attend(z_near(k) * n_x, n_x, start, many)

    mark("g_attown")
    attend_all(me, True)
    mark("g_pass0")
    pass_on(0)
    mark("g_pass1")
    pass_on(1)
    mark("fromy0")
    from_y(0)
    mark("kva")
    kv_forward(1, outward, False)
    mark("attownx")
    others_attend(my_z)
    loads[7].wait()
    loads[9].wait()
    loads[10].wait()
    loads[11].wait()
    mark("in0")
    row_scale = expert_in(0)
    mark("kvb")
    kv_forward(1, -outward, True)
    mark("hid0")
    expert_hidden(0, row_scale)
    mark("fromy1")
    from_y(1)
    mark("pass2")
    pass_on(2)
    mark("down0")
    expert_down(0)
    mark("in1")
    row_scale = expert_in(1)
    mark("kvf1")
    kv_forward(1, -outward, False)
    mark("hid1")
    expert_hidden(1, row_scale)
    mark("pass3")
    pass_on(3)
    mark("down1")
    expert_down(1)
    mark("att1")
    attend_first(1, others)
    mark("send0")
    expert_send(0)
    mark("kvf2")
    kv_forward(2, -outward, False)
    for s in range(2, n_z):
        if s > 2:
            mark(f"pass{s+1}")
            if s + 1 < n_z:
                pass_on(s + 1)
        mark(f"fromy{s}")
        from_y(s)
        mark(f"kvf{s}")
        if s < n_z // 2:
            kv_forward(s, outward, False)
        if 2 < s < n_z - 1:
            kv_forward(s, -outward, False)
        if s == 2:
            mark("att1x")
            near_arrived(1)
            attend_second(1, others)
        if s == n_z - 1:
            mark(f"kvg{s}")
            kv_forward(s, -outward, True)
        if s == 3:
            mark("att2")
            attend_first(2, others)
        mark(f"send{s-1}")
        expert_send(s - 1)
        mark(f"in{s}")
        row_scale = expert_in(s)
        mark(f"hid{s}")
        expert_hidden(s, row_scale)
        mark(f"down{s}")
        expert_down(s)
        if s < n_z - 1:
            mark(f"kvg{s}")
            kv_forward(s, -outward, True)
    mark("att2x")
    near_arrived(2)
    attend_second(2, others)
    mark("send")
    expert_send(n_z - 1)
    mark("ret0")
    expert_return(0)
    expert_return(1)
    loads[12].wait()
    mark("arr3")
    for k in range(3, n_z):
        near_arrived(k)
    for whose in (1 - core, core):
        if whose is core:
            mark("ret2")
            for o in range(2, n_z - 1):
                expert_return(o)
        for owner in others:
            mark("att3")
            for k in range(3, n_z):
                attend_both(k, owner * piece + whose * half, half)
            mark("mix")
            mix(owner, whose)
            if whose is not core:
                mix_mate(owner, 1 - core).start()
    mark("k_mixsum")
    for j in range(1, n_y):
        ms_out[y_peer(j)] = mix_sum(y_peer(j)).astype(BF)
        for c in range(pieces):
            mix_y(j, my_y, c).start()
    mark("k_ret")
    expert_return(n_z - 1)
    mark("k_att2")

    for k in range(1, n_z):
        attend_both(k, my_y * piece, piece)
    mark("k_mix")
    mix(my_y, 1 - core)
    mix_mate(my_y, 1 - core).start()
    mix(my_y, core)

    mark("n_mixsum")
    total = mix_sum(my_y)

    mark("l_retwait")

    def ret_wait(o, carry):
        source = (me + n_ep - o) % n_ep
        ret(source, source).wait_recv()
        return carry

    lax.fori_loop(1, n_ep, ret_wait, 0)
    mark("m_combine")
    loads[8].wait()
    back = ret_in[...].reshape(slots, col_w)
    share_row = scores_ref[...] / jnp.sum(scores_ref[...], axis=0, keepdims=True)
    own_token = lax.broadcasted_iota(jnp.int32, (tokens, tokens), 0) == lax.broadcasted_iota(
        jnp.int32, (tokens, tokens), 1
    )
    share_a, share_b = (
        jnp.sum(jnp.where(own_token, share_row[i:i + 1, :], 0.0), axis=1, keepdims=True)
        for i in range(2)
    )
    rows_a = lax.dot_general(
        pick_a, back, (((0,), (0,)), ((), ())), preferred_element_type=F32
    )
    rows_b = lax.dot_general(
        pick_b, back, (((0,), (0,)), ((), ())), preferred_element_type=F32
    )
    out_ref[...] = (rows_a * share_a + rows_b * share_b).astype(BF)

    mark("o_sends")

    def sends(o, carry):
        peer = (me + o) % n_ep
        disp(peer, me).wait_send()
        ret(peer, me).wait_send()
        return carry

    lax.fori_loop(1, n_ep, sends, 0)
    for i in range(1, n_x):

        def sent_x(z, carry):
            kv_send(x_peer(i), z * n_x + my_x, kvx_s.at[z, i]).wait_send()
            return carry

        lax.fori_loop(0, n_z, sent_x, 0)

    @pl.when(my_z < n_z - 1)
    def _():
        own_kv_right().wait_send()

    @pl.when(my_z > 0)
    def _():
        own_kv_left().wait_send()

    for t in range(1, n_z):
        for way in (outward, -outward):
            there, beyond, z, onward = kv_pass(t, way)

            @pl.when(jnp.logical_and(there, beyond))
            def _():
                onward.wait_send()

    for j in range(1, n_y):

        def sent_y(source, carry):
            over_y(j, source, my_y).wait_send()
            return carry

        lax.fori_loop(0, n_ep, sent_y, 0)
    for j in range(n_y):
        for s in range(stages):
            to_mate(y_peer(j), core, s).wait_send()
        for o in range(n_z):
            expert_mate(y_peer(j), 1 - core, o).wait_send()
            if j:
                expert_y(j, my_y, o).wait_send()
        mix_mate(y_peer(j), 1 - core).wait_send()

    mark("n_ywait")
    for j in range(1, n_y):
        for c in range(pieces):
            mix_y(j, y_peer(j), c).wait_recv()
        total = total + my_in[y_peer(j)].astype(F32)
    mark("n_out")
    mixed_ref[...] = total.astype(BF)
    for j in range(1, n_y):
        for c in range(pieces):
            mix_y(j, my_y, c).wait_send()
    mark(None)


def local(
    n_ep, n_tp,
    queries, key_input, value_input, query_gain, key_gain, mix_out_weight, expert_input, ffn_gain,
    routes, route_scores, gate_weight, up_weight, down_weight,
):
    rows = queries.shape[0]
    heads = queries.shape[1] // HD
    n_y = n_tp // 2
    n_x = 1 << ((n_ep.bit_length() - 1) // 2)
    n_z = n_ep // n_x
    stages = n_z
    spare = heads % 2 * HD
    if spare:
        queries = jnp.pad(queries, ((0, 0), (0, spare)))
        mix_out_weight = jnp.pad(mix_out_weight, ((0, spare), (0, 0)))
    width = expert_input.shape[1]
    col_w = width // n_tp
    tokens, top = routes.shape
    capacity = 3 * tokens * top // (2 * n_ep)
    slots_per = -(-capacity // 16) * 16
    slots = n_ep * slots_per
    hidden_w = gate_weight.shape[2]
    out_w = mix_out_weight.shape[1]
    half = rows // n_tp
    vm = pltpu.VMEM
    dma = pltpu.SemaphoreType.DMA
    scratch = [
        vm(queries.shape, BF), vm((rows, LANES), BF), vm((rows, LANES), BF), vm((tokens, col_w), BF),
        vm((1, HD), F32), vm((1, HD), F32), vm((1, width), F32), vm((top, tokens), jnp.int32), vm((top, tokens), F32),
        vm((width, hidden_w), BF), vm((width, hidden_w), BF), vm((hidden_w, width), BF),
        vm(mix_out_weight.shape, BF),
        vm((n_ep, rows, LANES), BF), vm((heads, rows, LANES), BF), vm((heads, rows, LANES), F32),
        vm((n_ep, slots_per, col_w), BF), vm((n_tp, n_ep, slots_per, col_w), BF),
        vm((slots, width), BF), vm((slots, hidden_w), BF),
        vm((n_tp, slots, col_w), BF), vm((n_y, slots, col_w), BF), vm((n_y, slots, col_w), BF),
        vm((n_y, slots, col_w), BF),
        vm((n_ep, slots_per, col_w), BF), vm((n_ep, slots_per, col_w), BF),
        vm((n_y, 2, half, out_w), BF), vm((n_y, half, out_w), BF), vm((n_y, half, out_w), BF),
        vm((n_y, half, out_w), BF),
        dma((13,)),
        dma((n_z, n_x)), dma((n_z, 2)), dma((n_ep,)), dma((n_ep,)), dma((n_ep,)),
        dma((n_y, n_ep)), dma((n_y, n_ep)),
    ] + [dma((n_y, stages))] * 2 + [dma((n_y, n_z))] * 4 + [dma((n_ep,))] * 2 + [dma((n_y,))] * 2 + [dma((n_y, 2))] * 2
    in_vmem = pl.BlockSpec(memory_space=pltpu.VMEM)
    in_hbm = pl.BlockSpec(memory_space=pltpu.HBM)
    return pl.pallas_call(
        functools.partial(kernel, n_ep, n_tp, heads, width),
        out_shape=(
            pltpu.VMEM((half, out_w), BF),
            pltpu.VMEM((tokens, col_w), BF),
        ),
        in_specs=[in_hbm] * 13,
        out_specs=(in_vmem, in_vmem),
        scratch_shapes=scratch,
        compiler_params=pltpu.CompilerParams(
            collective_id=0, has_side_effects=True, vmem_limit_bytes=56 * 1024 * 1024
        ),
    )(
        queries, key_input, value_input, query_gain[None, :], key_gain[None, :],
        mix_out_weight, expert_input, ffn_gain[None, :], routes.T, route_scores.T,
        gate_weight, up_weight, down_weight,
    )


def solution(mesh):
    placed = (
        P("ep", "tp"),
        P("ep", None),
        P("ep", None),
        P(),
        P(),
        P("tp", None),
        P("ep", None),
        P(),
        P("ep", None),
        P("ep", None),
        P("ep", None, "tp"),
        P("ep", None, "tp"),
        P("ep", "tp", None),
    )
    return jax.shard_map(
        functools.partial(local, mesh.shape["ep"], mesh.shape["tp"]),
        mesh=mesh,
        in_specs=placed,
        out_specs=(P(("ep", "tp"), None), P("ep", "tp")),
        check_vma=False,
    )
```
